512 devices in a mesh: sp: 32 (over z, x), tp: 16 (over y, core).
Axes of the slice: x: 4, y: 8, z: 8, core: 2. Of those that a mesh axis runs over, the one named last changes fastest.
Arguments:
- residual: bfloat16 [6144, 2048], P(('sp', 'tp')), may hold values from -6 to 6
- query_a: bfloat16 [6144, 1536], P('sp', 'tp'), may hold values from -600 to 600
- query_b: bfloat16 [6144, 2560], P('sp', 'tp'), may hold values from -600 to 600
- latents: bfloat16 [6144, 512], P('sp'), may hold values from -6 to 6
- rope_key: bfloat16 [6144, 32], P('sp'), may hold values from -6 to 6
- key_up_a: bfloat16 [512, 1024], P(None, 'tp'), may hold values from -0.25 to 0.25
- value_up_a: bfloat16 [512, 1024], P(None, 'tp'), may hold values from -0.25 to 0.25
- key_up_b: bfloat16 [512, 2048], P(None, 'tp'), may hold values from -0.25 to 0.25
- value_up_b: bfloat16 [512, 2048], P(None, 'tp'), may hold values from -0.25 to 0.25
- out_proj_a: bfloat16 [1024, 2048], P('tp'), may hold values from -1.5 to 1.5
- out_proj_b: bfloat16 [2048, 2048], P('tp'), may hold values from -1.5 to 1.5
- norm_gain: float32 [2048], replicated, may hold values from 0.1 to 1.9
- routes: int32 [6144, 2], P('sp'), may hold values from 0 to 31, all different within a row; in each aligned block of 192 rows (0 to 191, 192 to 383, ...) at most 18 rows name the same one
- route_weights: float32 [6144, 2], P('sp'), may hold values from 0.2 to 1
- shared_gate: bfloat16 [2048, 2048], P(None, 'tp'), may hold values from -0.125 to 0.125
- shared_up: bfloat16 [2048, 2048], P(None, 'tp'), may hold values from -0.125 to 0.125
- shared_down: bfloat16 [2048, 2048], P('tp'), may hold values from -0.125 to 0.125
- expert_gate: bfloat16 [32, 2048, 2048], P('sp', None, 'tp'), may hold values from -0.125 to 0.125
- expert_up: bfloat16 [32, 2048, 2048], P('sp', None, 'tp'), may hold values from -0.125 to 0.125
- expert_down: bfloat16 [32, 2048, 2048], P('sp', 'tp'), may hold values from -0.125 to 0.125
Outputs:
- layer_out: bfloat16 [6144, 2048], P(('sp', 'tp'))
The draws below stay inside these ranges and needn't reach their ends.
Inputs may be any that keep to these rules, and one draw needn't show every extreme that they name: `routes`: in each aligned block of 192 rows, no expert is named by more than 18 rows, a bound that some block reaches; a row names 2 different experts.
All inputs are finite; a program needn't handle non-finite values.
Results may differ from the reference program's by a relative error of at most 0.022.
The reference program's roundings to bfloat16 on the way count: a program that leaves them out, or rounds other values in their place, can miss the bound.
Values may be sent and summed in bfloat16 or wider, within the bound.
A program may use at most 64 MiB of HBM per device.

```python
import math
import jax
import jax.numpy as jnp
import numpy as np
from jax import lax

D = 2048
HA = 16
HB = 16
DA = 64
VA = 64
DB = 128
VB = 128
ROPE = 32
KV_RANK = 512
EXPERT_FF = 2048
SHARED_FF = 2048
TOPK = 2
TOK_DEV = 192
TOKENS = 6144
EXPERTS = 32
CAP = 18
N_SP = 32
N_TP = 16


def drawn_queries(key, width):
    base = jax.random.normal(key, (TOKENS, width), jnp.float32)
    return jnp.clip(base, -600.0, 600.0).astype(jnp.bfloat16)


def draw_query_a(key, part):
    return drawn_queries(jax.random.fold_in(key, 11), HA * (DA + ROPE))


def draw_query_b(key, part):
    return drawn_queries(jax.random.fold_in(key, 23), HB * (DB + ROPE))


def shard_levels(key, shape, cuts, smallest, top_value):
    def one(position, blocks):
        steps = jax.random.uniform(jax.random.fold_in(jax.random.fold_in(key, 6), position), (blocks,), jnp.float32, smallest / len(cuts), top_value / len(cuts))
        return jnp.repeat(jnp.exp(steps), shape[position] // blocks).reshape((-1,) + (1,) * (len(shape) - position - 1))

    loudness = one(*cuts[0])
    for cut in cuts[1:]:
        loudness = loudness * one(*cut)
    return loudness


def shared_out(stream_key, own, number, rows, amount, top, most, slope):
    ranking = jax.random.permutation(stream_key, amount)
    heavy_load, ordinary = load_shares(amount, rows * top, most, slope, True), load_shares(amount, rows * top, most, slope, False)
    places = jnp.arange(amount)

    def named(sizes, offset_by):
        used = int((sizes > 0).sum())
        fixed = max(1, used // 4)
        passed = fixed + (places - fixed + offset_by * (used - fixed)) % max(1, amount - fixed)
        return jnp.zeros((amount,), jnp.int32).at[ranking[jnp.where(places < fixed, places, passed)]].set(jnp.asarray(sizes, jnp.int32))

    sizes = jnp.where(number % 4 == 0, named(heavy_load, number // 4), named(ordinary, number - number // 4 - 1))
    mixed = jax.random.permutation(jax.random.fold_in(own, 3), amount)
    giver, sink = mixed[0:amount // 2 * 2:2], mixed[1:amount // 2 * 2:2]
    slack = jnp.minimum(sizes[giver] - 1, most - sizes[sink]) // 2
    slack = jnp.where((giver == ranking[0]) | (sink == ranking[0]) | (sizes[sink] == 0), 0, jnp.maximum(slack, 0))
    passed = jax.random.randint(jax.random.fold_in(own, 4), (amount // 2,), 0, 1 << 20) % (slack + 1)
    sizes = sizes.at[giver].add(-passed).at[sink].add(passed)
    labels = jnp.searchsorted(jnp.cumsum(sizes), jnp.arange(rows * top), side="right").astype(jnp.int32)
    listing = labels.reshape(top, rows).T
    listing = listing[jax.random.permutation(jax.random.fold_in(own, 1), rows)]
    offset_by = jax.random.randint(jax.random.fold_in(own, 2), (rows, 1), 0, top)
    return jnp.take_along_axis(listing, (jnp.arange(top)[None, :] + offset_by) % top, axis=1)


def load_shares(number_of, total, limit, skew, full):
    loads = [(1 << 20) // math.isqrt(standing ** skew) + 1 for standing in range(1, number_of + 1)]
    largest = limit if full else min(limit, max(-(-total // number_of), total * loads[0] // sum(loads)))
    least = 1 if total - largest >= number_of - 1 else 0
    given, surplus = [largest] + [least] * (number_of - 1), total - largest - least * (number_of - 1)
    while surplus > 0:
        candidates = [i for i in range(1, number_of) if given[i] < largest] or [i for i in range(1, number_of) if given[i] < limit]
        whole, remaining = sum([loads[i] for i in candidates]), surplus
        for i in candidates:
            addition = min(limit - given[i], max(1, remaining * loads[i] // whole), surplus)
            given[i] = given[i] + addition
            surplus = surplus - addition
    return np.array(given)


def bell_draw(stream_key, extent, spread, most, shards=(), kind=jnp.bfloat16):
    gain = shard_levels(stream_key, extent, shards, -0.22, 0.18) if shards else 1.0
    values = jax.random.normal(stream_key, extent, jnp.float32) * spread * gain
    return jnp.minimum(jnp.maximum(values, -most), most).astype(kind)


def setup_inputs(seed: int = 0) -> dict:
    arg_keys = jax.random.split(jax.random.key(seed), 21)
    residual = bell_draw(arg_keys[0], (TOKENS, D), 1.0, 6.0, ((0, 512),))
    query_a = draw_query_a(jax.random.fold_in(arg_keys[20], 71), 0)
    query_b = draw_query_b(jax.random.fold_in(arg_keys[20], 71), 0)
    latents = bell_draw(arg_keys[3], (TOKENS, KV_RANK), 1.0, 6.0, ((0, 32),))
    rope_key = bell_draw(arg_keys[4], (TOKENS, ROPE), 1.0, 6.0, ((0, 32),))
    key_up_a = bell_draw(arg_keys[5], (KV_RANK, HA * DA), KV_RANK ** -0.5, 0.25, ((1, 16),))
    value_up_a = bell_draw(arg_keys[6], (KV_RANK, HA * VA), KV_RANK ** -0.5, 0.25, ((1, 16),))
    key_up_b = bell_draw(arg_keys[7], (KV_RANK, HB * DB), KV_RANK ** -0.5, 0.25, ((1, 16),))
    value_up_b = bell_draw(arg_keys[8], (KV_RANK, HB * VB), KV_RANK ** -0.5, 0.25, ((1, 16),))
    out_proj_a = bell_draw(arg_keys[9], (HA * VA, D), HA ** -0.5, 1.5, ((0, 16),))
    out_proj_b = bell_draw(arg_keys[10], (HB * VB, D), HA ** -0.5, 1.5, ((0, 16),))
    norm_gain = jnp.clip(1.0 + 0.18 * jax.random.normal(arg_keys[11], (D,), jnp.float32), 0.1, 1.9)
    routes_keys = jax.random.split(jax.random.fold_in(arg_keys[12], 1), TOKENS // TOK_DEV)
    routes_turns = jax.random.permutation(jax.random.fold_in(arg_keys[12], 3), TOKENS // TOK_DEV)
    routes = jax.vmap(lambda own, number: shared_out(jax.random.fold_in(arg_keys[12], 2), own, number, TOK_DEV, EXPERTS, TOPK, CAP, 1))(routes_keys, routes_turns).reshape((TOKENS, TOPK))
    route_weights = jnp.clip(0.2 + 0.8 * jax.random.uniform(arg_keys[13], (TOKENS, TOPK), jnp.float32) ** shard_levels(arg_keys[13], (TOKENS, TOPK), ((0, 32),), -0.2, 0.2), 0.2, 1.0)
    shared_gate = bell_draw(arg_keys[14], (D, SHARED_FF), D ** -0.5, 0.125, ((1, 16),))
    shared_up = bell_draw(arg_keys[15], (D, SHARED_FF), D ** -0.5, 0.125, ((1, 16),))
    shared_down = bell_draw(arg_keys[16], (SHARED_FF, D), SHARED_FF ** -0.5, 0.125, ((0, 16),))
    expert_gate = bell_draw(arg_keys[17], (EXPERTS, D, EXPERT_FF), D ** -0.5, 0.125, ((0, 32), (2, 16)))
    expert_up = bell_draw(arg_keys[18], (EXPERTS, D, EXPERT_FF), D ** -0.5, 0.125, ((0, 32), (2, 16)))
    expert_down = bell_draw(arg_keys[19], (EXPERTS, EXPERT_FF, D), EXPERT_FF ** -0.5, 0.125, ((0, 32), (1, 16)))
    return dict(residual=residual, query_a=query_a, query_b=query_b, latents=latents, rope_key=rope_key, key_up_a=key_up_a, value_up_a=value_up_a, key_up_b=key_up_b, value_up_b=value_up_b, out_proj_a=out_proj_a, out_proj_b=out_proj_b, norm_gain=norm_gain, routes=routes, route_weights=route_weights, shared_gate=shared_gate, shared_up=shared_up, shared_down=shared_down, expert_gate=expert_gate, expert_up=expert_up, expert_down=expert_down)


theta_base = 10000.0
norm_eps = 1e-06

def round_trip(values):
    return lax.optimization_barrier(values.astype(jnp.bfloat16)).astype(jnp.float32)

def tables(positions):
    half = ROPE // 2
    freqs = theta_base ** (-(2.0 * jnp.arange(half, dtype=jnp.float32)) / ROPE)
    angles = positions.astype(jnp.float32)[:, None] * freqs[None, :]
    return (jnp.cos(angles), jnp.sin(angles))

def rotate(values, cosine, sine):
    half = values.shape[-1] // 2
    first = values[..., :half].astype(jnp.float32)
    second = values[..., half:].astype(jnp.float32)
    turned = jnp.concatenate([first * cosine - second * sine, first * sine + second * cosine], axis=-1)
    return turned.astype(jnp.bfloat16)

def attend(queries, keys, values, rot_key, heads, nope, vsize, cosine, sine):
    length = queries.shape[0]
    block = math.gcd(length, 512)
    shaped = queries.reshape(length, heads, nope + ROPE)
    q_nope = shaped[..., :nope]
    q_rope = rotate(shaped[..., nope:], cosine[:, None, :], sine[:, None, :])
    key_all = keys.reshape(length, heads, nope).astype(jnp.float32)
    value_all = values.reshape(length, heads, vsize).astype(jnp.float32)
    rot_all = rot_key.astype(jnp.float32)
    scale = (nope + ROPE) ** (-0.5)
    key_pos = jnp.arange(length, dtype=jnp.int32)

    def one_block(index):
        start = (index * block).astype(jnp.int32)
        q_first = lax.dynamic_slice_in_dim(q_nope, start, block, 0).astype(jnp.float32)
        q_second = lax.dynamic_slice_in_dim(q_rope, start, block, 0).astype(jnp.float32)
        scores = jnp.einsum('qhd,khd->hqk', q_first, key_all) + jnp.einsum('qhr,kr->hqk', q_second, rot_all)
        scores = scores * scale
        query_pos = start + jnp.arange(block, dtype=jnp.int32)
        mask = key_pos[None, :] <= query_pos[:, None]
        top = lax.optimization_barrier(jnp.max(jnp.where(mask[None], scores, -jnp.inf), axis=-1, keepdims=True))
        expo = jnp.where(mask[None], jnp.exp(scores - top), 0.0)
        total = lax.optimization_barrier(jnp.sum(expo, axis=-1))
        weighted = jnp.einsum('hqk,khv->hqv', round_trip(expo), value_all)
        result = (weighted / total[..., None]).astype(jnp.bfloat16)
        return jnp.transpose(result, (1, 0, 2)).reshape(block, heads * vsize)
    blocks = lax.map(one_block, jnp.arange(length // block, dtype=jnp.int32))
    return blocks.reshape(length, heads * vsize)

def reference(residual, query_a, query_b, latents, rope_key, key_up_a, value_up_a, key_up_b, value_up_b, out_proj_a, out_proj_b, norm_gain, routes, route_weights, shared_gate, shared_up, shared_down, expert_gate, expert_up, expert_down):
    positions = jnp.arange(TOKENS, dtype=jnp.int32)
    cosine, sine = tables(positions)
    rot_key = rotate(rope_key, cosine, sine)
    keys_a = jnp.dot(latents, key_up_a, preferred_element_type=jnp.float32).astype(jnp.bfloat16)
    values_a = jnp.dot(latents, value_up_a, preferred_element_type=jnp.float32).astype(jnp.bfloat16)
    keys_b = jnp.dot(latents, key_up_b, preferred_element_type=jnp.float32).astype(jnp.bfloat16)
    values_b = jnp.dot(latents, value_up_b, preferred_element_type=jnp.float32).astype(jnp.bfloat16)
    heads_a = attend(query_a, keys_a, values_a, rot_key, HA, DA, VA, cosine, sine)
    heads_b = attend(query_b, keys_b, values_b, rot_key, HB, DB, VB, cosine, sine)
    width_a = HA * VA // N_TP
    width_b = HB * VB // N_TP

    def head_block(total, index):
        part = jnp.dot(lax.dynamic_slice_in_dim(heads_a, index * width_a, width_a, 1), lax.dynamic_slice_in_dim(out_proj_a, index * width_a, width_a, 0), preferred_element_type=jnp.float32)
        part = part + jnp.dot(lax.dynamic_slice_in_dim(heads_b, index * width_b, width_b, 1), lax.dynamic_slice_in_dim(out_proj_b, index * width_b, width_b, 0), preferred_element_type=jnp.float32)
        return (total + round_trip(part), None)
    mixed, _ = lax.scan(head_block, jnp.zeros((TOKENS, D), jnp.float32), jnp.arange(N_TP, dtype=jnp.int32))
    hidden_state = (residual.astype(jnp.float32) + mixed).astype(jnp.bfloat16)
    wide = hidden_state.astype(jnp.float32)
    normed = (wide * lax.rsqrt(lax.optimization_barrier(jnp.mean(wide * wide, axis=-1, keepdims=True)) + norm_eps) * norm_gain.astype(jnp.float32)).astype(jnp.bfloat16)
    flat = routes.reshape(-1).astype(jnp.int32)
    owners = jnp.arange(TOKENS * TOPK, dtype=jnp.int32) // TOPK
    weights_flat = route_weights.reshape(-1).astype(jnp.float32)
    bound = N_SP * CAP

    def select(expert):
        order = jnp.argsort(jnp.where(flat == expert, 0, 1).astype(jnp.int32), stable=True)[:bound].astype(jnp.int32)
        chosen = jnp.where(flat[order] == expert, weights_flat[order], 0.0)
        return (owners[order], chosen)
    rows_of, weight_of = lax.map(select, jnp.arange(EXPERTS, dtype=jnp.int32))
    expert_width = EXPERT_FF // N_TP
    shared_width = SHARED_FF // N_TP

    def width_block(total, index):
        s_gate = lax.dynamic_slice_in_dim(shared_gate, index * shared_width, shared_width, 1)
        s_up = lax.dynamic_slice_in_dim(shared_up, index * shared_width, shared_width, 1)
        s_down = lax.dynamic_slice_in_dim(shared_down, index * shared_width, shared_width, 0)
        act = (jax.nn.silu(jnp.dot(normed, s_gate, preferred_element_type=jnp.float32)) * jnp.dot(normed, s_up, preferred_element_type=jnp.float32)).astype(jnp.bfloat16)
        term = jnp.dot(act, s_down, preferred_element_type=jnp.float32)

        def one_expert(acc, pieces):
            gate_w, up_w, down_w, rows, weight = pieces
            taken = normed[rows]
            gate_blk = lax.dynamic_slice_in_dim(gate_w, index * expert_width, expert_width, 1)
            up_blk = lax.dynamic_slice_in_dim(up_w, index * expert_width, expert_width, 1)
            down_blk = lax.dynamic_slice_in_dim(down_w, index * expert_width, expert_width, 0)
            act_e = (jax.nn.silu(jnp.dot(taken, gate_blk, preferred_element_type=jnp.float32)) * jnp.dot(taken, up_blk, preferred_element_type=jnp.float32)).astype(jnp.bfloat16)
            part = round_trip(jnp.dot(act_e, down_blk, preferred_element_type=jnp.float32))
            return (acc.at[rows].add(part * weight[:, None]), None)
        term, _ = lax.scan(one_expert, term, (expert_gate, expert_up, expert_down, rows_of, weight_of))
        return (total + round_trip(term), None)
    moe, _ = lax.scan(width_block, jnp.zeros((TOKENS, D), jnp.float32), jnp.arange(N_TP, dtype=jnp.int32))
    return (hidden_state.astype(jnp.float32) + moe).astype(jnp.bfloat16)
```

```python
import functools

import jax
import jax.numpy as jnp
from jax import lax
from jax.experimental import pallas as pl
from jax.experimental.pallas import tpu as pltpu
from jax.sharding import Mesh
from jax.sharding import PartitionSpec as P

DA = 64
VA = 64
DB = 128
VB = 128
ROPE = 32
TOK = 192
D = 2048
W = 128
CAP = 18
CAPP = 24
NZ, NX, NY, NC = 4 * 2, 4, 8, 2
NSP = NZ * NX
NTP = NY * NC
ROWS = NSP * CAP
PROWS = NSP * CAPP
HALF = ROWS // 2
OWN = TOK // NTP
OWNP = 16
SP = ("z", "x")
TP = ("y", "c")
ALL = ("z", "x", "y", "c")
MESH_ID = pl.DeviceIdType.MESH
F32 = jnp.float32
BF16 = jnp.bfloat16
FAR_FIRST = (4, 3, 5, 2, 6, 1, 7, 0)

theta_base = 10000.0
norm_eps = 1e-06
very_low = -1e30


def fdot(a, b):
    return jnp.dot(a, b, preferred_element_type=F32)


def rcopy(src, dst, ssem, rsem, dev):
    return pltpu.make_async_remote_copy(
        src_ref=src, dst_ref=dst, send_sem=ssem, recv_sem=rsem, device_id=dev, device_id_type=MESH_ID
    )


def iota(shape, dim):
    return lax.broadcasted_iota(jnp.int32, shape, dim)


def onehot(cond):
    return jnp.where(cond, 1.0, 0.0).astype(BF16)


def lanes(index, width):
    return pl.ds(pl.multiple_of(index * width, 128), width)


def post_kernel(
    heads_a, heads_b, resid, gain, routes, routes_t, rw,
    oa_h, ob_h, sg_h, su_h, sd_h, eg_h, eu_h, ed_h,
    out,
    oa, ob, sgu, sd, egu, ed,
    r_r, own_d, po_d, pi_d, sb_d, rb_d,
    hs, hfull, normed,
    po_s, pi_s, sb_s, rb_s, own_s,
    f_s, f_r, comp, expd, g, hacc,
    own_i, po_i, pi_i, isb, irb, j_r, l_s, l_r,
    w_sem, r_ss, r_rs, pd_ss, pd_rs, d_ss, d_rs, e_ss, e_rs, ef_ss, ef_rs,
    ps_ss, ps_rs, s_ss, s_rs, f_ss, f_rs, g_ss, g_rs, gf_ss, gf_rs, go_ss, go_rs,
    pp_ss, pp_rs, i_ss, i_rs, j_ss, j_rs, l_ss, l_rs,
):
    z, x, y, c = (lax.axis_index(a) for a in ALL)
    t = y * NC + c
    sp = z * NX + x
    oc = 1 - c
    partner = (z, x, y, oc)

    def ydev(yy):
        return (z, x, yy, c)

    def tdev(tt):
        return (z, x, tt // NC, lax.rem(tt, NC))

    def sdev(ss):
        return (ss // NX, lax.rem(ss, NX), y, c)

    def yoff(off):
        return lax.rem(y + off, NY)

    weights = [
        (oa_h, oa), (ob_h, ob), (sg_h, sgu.at[:, 0:W]), (su_h, sgu.at[:, W:2 * W]), (sd_h, sd),
        (eg_h, egu.at[:, 0:W]), (eu_h, egu.at[:, W:2 * W]), (ed_h, ed),
    ]
    loads = [pltpu.make_async_copy(a, b, w_sem.at[i]) for i, (a, b) in enumerate(weights)]
    for load in loads:
        load.start()

    barrier = pltpu.get_barrier_semaphore()

    def greet_t(k, _):
        pl.semaphore_signal(barrier, inc=1, device_id=tdev(lax.rem(t + k, NTP)), device_id_type=MESH_ID)
        return 0

    def greet_s(k, _):
        pl.semaphore_signal(barrier, inc=1, device_id=sdev(lax.rem(sp + k, NSP)), device_id_type=MESH_ID)
        return 0

    lax.fori_loop(1, NTP, greet_t, 0)
    lax.fori_loop(1, NSP, greet_s, 0)

    names = onehot((iota((TOK, 128), 1) == routes[:, 0:1]) | (iota((TOK, 128), 1) == routes[:, 1:2]))
    lower = onehot(iota((TOK, TOK), 0) > iota((TOK, TOK), 1))
    before = fdot(lower, names)
    names_t = onehot((iota((128, TOK), 0) == routes_t[0:1, :]) | (iota((128, TOK), 0) == routes_t[1:2, :]))
    upper = onehot(iota((TOK, TOK), 0) < iota((TOK, TOK), 1))
    before_t = fdot(names_t, upper)

    def slot_col(k):
        rank = jnp.sum(jnp.where(iota((TOK, 128), 1) == routes[:, k:k + 1], before, 0.0), axis=1, keepdims=True)
        return routes[:, k:k + 1] * CAPP + rank.astype(jnp.int32)

    def slot_row(k):
        rank = jnp.sum(jnp.where(iota((128, TOK), 0) == routes_t[k:k + 1, :], before_t, 0.0), axis=0, keepdims=True)
        return routes_t[k:k + 1, :] * CAPP + rank.astype(jnp.int32)

    i_col = iota((ROWS, 1), 0)
    comp[...] = onehot(iota((ROWS, PROWS), 1) == i_col + (CAPP - CAP) * ((i_col * 3641) >> 16))
    j_col = iota((PROWS, 1), 0)
    j_q = (j_col * 2731) >> 16
    j_r0 = j_col - CAPP * j_q
    expd[...] = onehot(iota((PROWS, ROWS), 1) == jnp.where(j_r0 < CAP, CAP * j_q + j_r0, -1))

    loads[0].wait()
    loads[1].wait()
    pl.semaphore_wait(barrier, NTP - 1 + NSP - 1)

    def resid_copy(k, to):
        tt = lax.rem(t + k, NTP) if to else lax.rem(t + NTP - k, NTP)
        return rcopy(resid.at[:, lanes(tt if to else t, W)], r_r.at[t if to else tt], r_ss.at[k], r_rs.at[k], tdev(tt))

    def resid_send(k, _):
        resid_copy(k, True).start()
        return 0

    r_r[t] = resid[:, lanes(t, W)]

    def pair_out(value, off, own, po, pi, ss, rs):
        left, right = value[:, 0:W], value[:, W:2 * W]
        own[off] = jnp.where(c == 0, left, right)
        po[off] = jnp.where(c == 0, right, left).astype(BF16)
        rcopy(po.at[off], pi.at[off], ss.at[off], rs.at[off], partner).start()

    def pair_wait(off, po, pi, ss, rs):
        rcopy(po.at[off], pi.at[off], ss.at[off], rs.at[off], partner).wait()

    def y_copy(off, sb, rb, ss, rs):
        return rcopy(sb.at[off], rb.at[off], ss.at[off], rs.at[off], ydev(yoff(off)))

    def scatter_start(cols, own, po, pi, sb, rb, pss, prs, ss, rs, lead=3):
        for n in range(NY + lead):
            if n < NY:
                off = FAR_FIRST[n]
                pair_out(cols(yoff(off)), off, own, po, pi, pss, prs)
            if n >= lead:
                off = FAR_FIRST[n - lead]
                pair_wait(off, po, pi, pss, prs)
                if off:
                    sb[off] = (own[off] + pi[off].astype(F32)).astype(BF16)
                    y_copy(off, sb, rb, ss, rs).start()

    def scatter_end(own, pi, sb, rb, ss, rs):
        total = own[0] + pi[0].astype(F32)
        for off in range(1, NY):
            y_copy(off, sb, rb, ss, rs).wait()
            total = total + rb[off].astype(F32)
        return total

    def head_cols(yy):
        cut = lanes(yy, 2 * W)
        return fdot(heads_a[...], oa[:, cut]) + fdot(heads_b[...], ob[:, cut])

    scatter_start(head_cols, own_d, po_d, pi_d, sb_d, rb_d, pd_ss, pd_rs, d_ss, d_rs)
    lax.fori_loop(1, NTP, resid_send, 0)

    def resid_wait(k, _):
        resid_copy(k, False).wait()
        return 0

    mixed = scatter_end(own_d, pi_d, sb_d, rb_d, d_ss, d_rs)
    lax.fori_loop(1, NTP, resid_wait, 0)
    i12 = iota((TOK, 1), 0)
    pick12 = onehot(iota((TOK, NTP * OWNP), 1) == i12 + (OWNP - OWN) * ((i12 * 5462) >> 16))
    resid_cols = fdot(pick12, r_r[...].reshape(NTP * OWNP, W))
    hs[...] = (resid_cols + mixed).astype(BF16)

    hfull[:, lanes(t, W)] = hs[...]

    def e_copy(off):
        return rcopy(hs, hfull.at[:, lanes(t, W)], e_ss.at[off], e_rs.at[off], ydev(yoff(off)))

    def e_got(off):
        src = lanes(lax.rem(y + NY - off, NY) * NC + c, W)
        return rcopy(hs, hfull.at[:, src], e_ss.at[off], e_rs.at[off], ydev(yoff(off)))

    def e_fwd(off, core):
        win = hfull.at[:, lanes(lax.rem(y + NY - off, NY) * NC + core, W)]
        return rcopy(win, win, ef_ss.at[off], ef_rs.at[off], partner)

    for off in FAR_FIRST[:-1]:
        e_copy(off).start()
    e_fwd(0, c).start()
    for off in (1, 7, 2, 6, 3, 5, 4):
        e_got(off).wait_recv()
        e_fwd(off, c).start()
    for off in range(NY):
        e_fwd(off, oc).wait_recv()

    def norm_rows(b, _):
        rows = pl.ds(pl.multiple_of(b * 16, 16), 16)
        wide = hfull[rows, :].astype(F32)
        mean = jnp.mean(wide * wide, axis=-1, keepdims=True)
        normed[rows, :] = (wide * lax.rsqrt(mean + norm_eps) * gain[...]).astype(BF16)
        return 0

    lax.fori_loop(0, TOK // 16, norm_rows, 0)

    place = onehot((iota((PROWS, TOK), 0) == slot_row(0)) | (iota((PROWS, TOK), 0) == slot_row(1)))
    f_s[...] = fdot(place, normed[:, lanes(t, W)]).reshape(NSP, CAPP, W).astype(BF16)
    f_r[sp] = f_s[sp]

    def sp_copy(k, src, dst, ss, rs, to):
        peer = lax.rem(sp + k, NSP) if to else lax.rem(sp + NSP - k, NSP)
        return rcopy(src.at[peer], dst.at[sp if to else peer], ss.at[k], rs.at[k], sdev(peer))

    def f_send(k, _):
        sp_copy(k, f_s, f_r, f_ss, f_rs, True).start()
        return 0

    def f_wait(k, _):
        sp_copy(k, f_s, f_r, f_ss, f_rs, False).wait()
        return 0

    lax.fori_loop(1, NSP, f_send, 0)

    for load in loads[2:]:
        load.wait()
    both = fdot(normed[...], sgu[...])
    gate, up = both[:, 0:W], both[:, W:2 * W]
    shared_act = (gate / (1.0 + jnp.exp(-gate)) * up).astype(BF16)

    def shared_cols(yy):
        return fdot(shared_act, sd[:, lanes(yy, 2 * W)])

    scatter_start(shared_cols, own_s, po_s, pi_s, sb_s, rb_s, ps_ss, ps_rs, s_ss, s_rs)

    lax.fori_loop(1, NSP, f_wait, 0)
    g[y, :, lanes(c, W)] = fdot(comp[...], f_r[...].astype(F32).reshape(PROWS, W).astype(BF16)).astype(BF16)

    def ok_g(d, k, h):
        return k < 4 or h == d

    def ysrc(d, k):
        return lax.rem(y + NY - k, NY) if d == 0 else lax.rem(y + k, NY)

    def ydst(d):
        return ydev(lax.rem(y + 1, NY) if d == 0 else lax.rem(y + NY - 1, NY))

    def g_win(yy, h, core):
        return g.at[yy, pl.ds(h * HALF, HALF), lanes(core, W)]

    def g_send(d, k, h):
        win = g_win(ysrc(d, k - 1), h, c)
        return rcopy(win, win, g_ss.at[d, k - 1, h], g_rs.at[d, k - 1, h], ydst(d))

    def g_got(d, k, h):
        win = g_win(ysrc(d, k), h, c)
        return rcopy(win, win, g_ss.at[d, k - 1, h], g_rs.at[d, k - 1, h], ydst(d))

    def g_fwd(d, k, h, core):
        win = g_win(ysrc(d, k), h, core)
        return rcopy(win, win, gf_ss.at[d, k - 1, h], gf_rs.at[d, k - 1, h], partner)

    def g_own(core):
        win = g.at[y, :, lanes(core, W)]
        return rcopy(win, win, go_ss, go_rs, partner)

    for h in range(2):
        for d in range(2):
            g_send(d, 1, h).start()
    g_own(c).start()

    def gate_up(yy, first=False):
        value = fdot(g[yy], egu[pl.ds(pl.multiple_of(yy * 2 * W, 2 * W), 2 * W), :])
        hacc[...] = value if first else hacc[...] + value

    for k in range(1, 5):
        for h in range(2):
            for d in range(2):
                if ok_g(d, k, h):
                    g_got(d, k, h).wait_recv()
                    if k < 4 and ok_g(d, k + 1, h):
                        g_send(d, k + 1, h).start()
                    g_fwd(d, k, h, c).start()
        if k == 1:
            g_own(oc).wait_recv()
            gate_up(y, True)
        else:
            for d in range(2):
                for h in range(2):
                    g_fwd(d, k - 1, h, oc).wait_recv()
                gate_up(ysrc(d, k - 1))
    g_fwd(0, 4, 0, oc).wait_recv()
    g_fwd(1, 4, 1, oc).wait_recv()
    gate_up(yoff(4))
    gate, up = hacc[:, 0:W], hacc[:, W:2 * W]
    act = (gate / (1.0 + jnp.exp(-gate)) * up).astype(BF16)

    def i_pair(off):
        pair_out(fdot(act, ed[:, lanes(yoff(off), 2 * W)]), off, own_i, po_i, pi_i, pp_ss, pp_rs)

    def i_copy(d, k, h):
        return rcopy(isb.at[d, k - 1, h], irb.at[d, k - 1, h], i_ss.at[d, k - 1, h], i_rs.at[d, k - 1, h], ydst(d))

    def i_step(k):
        for h in range(2):
            for d in range(2):
                if k > 1 or h == d:
                    off = (5 - k) if d == 0 else (3 + k)
                    rows = pl.ds(h * HALF, HALF)
                    total = own_i[off, rows, :] + pi_i[off, rows, :].astype(F32)
                    if k > 2 or (k == 2 and h == d):
                        i_copy(d, k - 1, h).wait_recv()
                        total = total + irb[d, k - 2, h].astype(F32)
                    isb[d, k - 1, h] = total.astype(BF16)
                    i_copy(d, k, h).start()

    i_pair(4)
    i_pair(3)
    i_pair(5)
    pair_wait(4, po_i, pi_i, pp_ss, pp_rs)
    i_step(1)
    i_pair(2)
    i_pair(6)
    pair_wait(3, po_i, pi_i, pp_ss, pp_rs)
    pair_wait(5, po_i, pi_i, pp_ss, pp_rs)
    i_step(2)
    i_pair(1)
    i_pair(7)
    i_pair(0)
    pair_wait(2, po_i, pi_i, pp_ss, pp_rs)
    pair_wait(6, po_i, pi_i, pp_ss, pp_rs)
    i_step(3)
    pair_wait(1, po_i, pi_i, pp_ss, pp_rs)
    pair_wait(7, po_i, pi_i, pp_ss, pp_rs)
    i_step(4)
    pair_wait(0, po_i, pi_i, pp_ss, pp_rs)
    for h in range(2):
        rows = pl.ds(h * HALF, HALF)
        total = own_i[0, rows, :] + pi_i[0, rows, :].astype(F32)
        for d in range(2):
            i_copy(d, 4, h).wait_recv()
            total = total + irb[d, 3, h].astype(F32)
        own_i[0, rows, :] = total

    f_s[...] = fdot(expd[...], own_i[0].astype(BF16)).reshape(NSP, CAPP, W).astype(BF16)
    j_r[sp] = f_s[sp]

    def j_send(k, _):
        sp_copy(k, f_s, j_r, j_ss, j_rs, True).start()
        return 0

    def j_wait(k, _):
        sp_copy(k, f_s, j_r, j_ss, j_rs, False).wait()
        return 0

    lax.fori_loop(1, NSP, j_send, 0)
    final = hs[...].astype(F32) + scatter_end(own_s, pi_s, sb_s, rb_s, s_ss, s_rs)
    lax.fori_loop(1, NSP, j_wait, 0)
    back = j_r[...].astype(F32).reshape(PROWS, W).astype(BF16)
    for k in range(2):
        pick = onehot(iota((TOK, PROWS), 1) == slot_col(k))
        final = final + fdot(pick, back) * rw[:, k:k + 1]

    j16 = iota((NTP * OWNP, 1), 0)
    spread = onehot(iota((NTP * OWNP, TOK), 1) == jnp.where((j16 & 15) < OWN, OWN * (j16 >> 4) + (j16 & 15), -1))
    l_s[...] = fdot(spread, final.astype(BF16)).astype(BF16).reshape(NTP, OWNP, W)
    l_r[:, lanes(t, W)] = l_s[t]

    def l_copy(k, to):
        tt = lax.rem(t + k, NTP) if to else lax.rem(t + NTP - k, NTP)
        return rcopy(l_s.at[tt], l_r.at[:, lanes(t if to else tt, W)], l_ss.at[k], l_rs.at[k], tdev(tt))

    def l_send(k, _):
        l_copy(k, True).start()
        return 0

    def l_wait(k, _):
        l_copy(k, False).wait()
        return 0

    lax.fori_loop(1, NTP, l_send, 0)
    for off in range(1, NY):
        e_copy(off).wait_send()
    for off in range(NY):
        e_fwd(off, c).wait_send()
    g_own(c).wait_send()
    for k in range(1, 5):
        for h in range(2):
            for d in range(2):
                if ok_g(d, k, h):
                    g_send(d, k, h).wait_send()
                    g_fwd(d, k, h, c).wait_send()
                if k > 1 or h == d:
                    i_copy(d, k, h).wait_send()
    lax.fori_loop(1, NTP, l_wait, 0)
    out[...] = l_r[...]


def post(heads_a, heads_b, residual, norm_gain, routes, route_weights, weights):
    resid = jnp.pad(residual, ((0, OWNP - OWN), (0, 0)))
    dma = pltpu.SemaphoreType.DMA
    vm = pltpu.VMEM
    scratch = [
        vm((64, D), BF16), vm((128, D), BF16), vm((D, 2 * W), BF16), vm((W, D), BF16), vm((D, 2 * W), BF16), vm((W, D), BF16),
        vm((NTP, OWNP, W), BF16), vm((NY, TOK, W), F32), vm((NY, TOK, W), BF16), vm((NY, TOK, W), BF16), vm((NY, TOK, W), BF16), vm((NY, TOK, W), BF16),
        vm((TOK, W), BF16), vm((TOK, D), BF16), vm((TOK, D), BF16),
        vm((NY, TOK, W), BF16), vm((NY, TOK, W), BF16), vm((NY, TOK, W), BF16), vm((NY, TOK, W), BF16), vm((NY, TOK, W), F32),
        vm((NSP, CAPP, W), BF16), vm((NSP, CAPP, W), BF16), vm((ROWS, PROWS), BF16), vm((PROWS, ROWS), BF16), vm((NY, ROWS, 2 * W), BF16), vm((ROWS, 2 * W), F32),
        vm((NY, ROWS, W), F32), vm((NY, ROWS, W), BF16), vm((NY, ROWS, W), BF16), vm((2, 4, 2, HALF, W), BF16), vm((2, 4, 2, HALF, W), BF16),
        vm((NSP, CAPP, W), BF16), vm((NTP, OWNP, W), BF16), vm((OWNP, D), BF16),
        dma((8,)), dma((NTP,)), dma((NTP,)), dma((NY,)), dma((NY,)), dma((NY,)), dma((NY,)), dma((NY,)), dma((NY,)), dma((NY,)), dma((NY,)),
        dma((NY,)), dma((NY,)), dma((NY,)), dma((NY,)), dma((NSP,)), dma((NSP,)),
        dma((2, 4, 2)), dma((2, 4, 2)), dma((2, 4, 2)), dma((2, 4, 2)), dma, dma,
        dma((NY,)), dma((NY,)), dma((2, 4, 2)), dma((2, 4, 2)), dma((NSP,)), dma((NSP,)), dma((NTP,)), dma((NTP,)),
    ]
    vspec = pl.BlockSpec(memory_space=pltpu.VMEM)
    hspec = pl.BlockSpec(memory_space=pl.ANY)
    padded = pl.pallas_call(
        post_kernel,
        out_shape=jax.ShapeDtypeStruct((OWNP, D), BF16),
        in_specs=[vspec] * 7 + [hspec] * 8,
        out_specs=vspec,
        scratch_shapes=scratch,
        compiler_params=pltpu.CompilerParams(collective_id=1, has_side_effects=True, vmem_limit_bytes=60 * 2**20),
        name="post",
    )(heads_a, heads_b, resid, norm_gain.reshape(1, D), routes, routes.T, route_weights, *weights)
    return padded[:OWN]


def sent_together(arrays, axis, dim, along):
    ends, at = ([], 0)
    for a in arrays[:-1]:
        at += a.shape[along]
        ends.append(at)
    both = jnp.concatenate(arrays, axis=along)
    return tuple(jnp.split(lax.all_gather(both, axis, axis=dim, tiled=True), ends, axis=along))


def tables(positions, width):
    half = width // 2
    freqs = theta_base ** (-(2.0 * jnp.arange(half, dtype=jnp.float32)) / width)
    angles = positions.astype(jnp.float32)[:, None] * freqs[None, :]
    return (jnp.cos(angles), jnp.sin(angles))


def rotate(values, cosine, sine):
    half = values.shape[-1] // 2
    first = values[..., :half].astype(jnp.float32)
    second = values[..., half:].astype(jnp.float32)
    turned = jnp.concatenate(
        [first * cosine - second * sine, first * sine + second * cosine], axis=-1
    )
    return turned.astype(jnp.bfloat16)


def group_update(state, queries_nope, queries_rope, keys, values, rot_piece, mask, scale):
    top, total, weighted = state
    scores = jnp.einsum("qhd,khd->hqk", queries_nope, keys, preferred_element_type=jnp.float32)
    scores = scores + jnp.einsum(
        "qhr,kr->hqk", queries_rope, rot_piece, preferred_element_type=jnp.float32
    )
    scores = jnp.where(mask[None], scores * scale, very_low)
    new_top = jnp.maximum(top, jnp.max(scores, axis=-1))
    expo = jnp.where(mask[None], jnp.exp(scores - new_top[..., None]), 0.0)
    total = jnp.sum(expo, axis=-1)
    weighted = jnp.einsum(
        "hqk,khv->hqv", expo.astype(jnp.bfloat16), values, preferred_element_type=jnp.float32
    )
    return (new_top, total, weighted)


def empty_state(heads, rows, vsize):
    return (
        jnp.full((heads, rows), very_low, jnp.float32),
        jnp.zeros((heads, rows), jnp.float32),
        jnp.zeros((heads, rows, vsize), jnp.float32),
    )


def shards(
    residual,
    query_a,
    query_b,
    latents,
    rope_key,
    key_up_a,
    value_up_a,
    key_up_b,
    value_up_b,
    out_proj_a,
    out_proj_b,
    norm_gain,
    routes,
    route_weights,
    shared_gate,
    shared_up,
    shared_down,
    expert_gate,
    expert_up,
    expert_down,
):
    tok = query_a.shape[0]
    heads_a = key_up_a.shape[1] // DA
    heads_b = key_up_b.shape[1] // DB
    first_row = lax.axis_index(SP) * tok
    last_row = first_row + tok
    query_pos = first_row + jnp.arange(tok, dtype=jnp.int32)
    cosine, sine = tables(query_pos, ROPE)
    rot_key = rotate(rope_key, cosine, sine)
    shaped_a = query_a.reshape(tok, heads_a, DA + ROPE)
    shaped_b = query_b.reshape(tok, heads_b, DB + ROPE)
    nope_a = shaped_a[..., :DA]
    nope_b = shaped_b[..., :DB]
    turned_a = rotate(shaped_a[..., DA:], cosine[:, None, :], sine[:, None, :])
    turned_b = rotate(shaped_b[..., DB:], cosine[:, None, :], sine[:, None, :])
    scale_a = (DA + ROPE) ** (-0.5)
    scale_b = (DB + ROPE) ** (-0.5)

    def attend(state, keys_a, values_a, keys_b, values_b, rot_piece, key_pos):
        count = keys_a.shape[0]
        mask = key_pos[None, :] <= query_pos[:, None]
        state_a = group_update(
            state[0],
            nope_a,
            turned_a,
            keys_a.reshape(count, heads_a, DA),
            values_a.reshape(count, heads_a, VA),
            rot_piece,
            mask,
            scale_a,
        )
        state_b = group_update(
            state[1],
            nope_b,
            turned_b,
            keys_b.reshape(count, heads_b, DB),
            values_b.reshape(count, heads_b, VB),
            rot_piece,
            mask,
            scale_b,
        )
        return (state_a, state_b)

    start_state = (empty_state(heads_a, tok, VA), empty_state(heads_b, tok, VB))
    keys_a = jnp.dot(latents, key_up_a, preferred_element_type=jnp.float32).astype(jnp.bfloat16)
    values_a = jnp.dot(latents, value_up_a, preferred_element_type=jnp.float32).astype(jnp.bfloat16)
    keys_b = jnp.dot(latents, key_up_b, preferred_element_type=jnp.float32).astype(jnp.bfloat16)
    values_b = jnp.dot(latents, value_up_b, preferred_element_type=jnp.float32).astype(jnp.bfloat16)
    keys_a, values_a, keys_b, values_b = (keys_a, values_a, keys_b, values_b)
    piece = sent_together((keys_a, values_a, keys_b, values_b, rot_key), SP, 0, 1)
    key_pos = jnp.arange(piece[0].shape[0], dtype=jnp.int32)

    def compute(inner):
        return attend(inner, piece[0], piece[1], piece[2], piece[3], piece[4], key_pos)

    state = lax.cond(jnp.int32(0) < last_row, compute, lambda inner: inner, start_state)
    heads_out_a = (state[0][2] / state[0][1][..., None]).astype(jnp.bfloat16)
    heads_out_b = (state[1][2] / state[1][1][..., None]).astype(jnp.bfloat16)
    heads_out_a = heads_out_a.transpose(1, 0, 2).reshape(tok, heads_a * VA)
    heads_out_b = heads_out_b.transpose(1, 0, 2).reshape(tok, heads_b * VB)
    weights = (
        out_proj_a, out_proj_b, shared_gate, shared_up, shared_down,
        expert_gate[0], expert_up[0], expert_down[0],
    )
    return post(heads_out_a, heads_out_b, residual, norm_gain, routes, route_weights, weights)


def solution(mesh):
    torus = Mesh(mesh.devices.reshape(NZ, NX, NY, NC), ALL)
    in_specs = (
        P(SP + TP, None),
        P(SP, TP),
        P(SP, TP),
        P(SP, None),
        P(SP, None),
        P(None, TP),
        P(None, TP),
        P(None, TP),
        P(None, TP),
        P(TP, None),
        P(TP, None),
        P(),
        P(SP, None),
        P(SP, None),
        P(None, TP),
        P(None, TP),
        P(TP, None),
        P(SP, None, TP),
        P(SP, None, TP),
        P(SP, TP, None),
    )
    return jax.shard_map(
        shards, mesh=torus, in_specs=in_specs, out_specs=P(SP + TP, None), check_vma=False
    )
```

```python
import functools

import jax
import jax.numpy as jnp
from jax import lax
from jax.experimental import pallas as pl
from jax.experimental.pallas import tpu as pltpu
from jax.sharding import Mesh
from jax.sharding import PartitionSpec as P

DA = 64
VA = 64
DB = 128
VB = 128
ROPE = 32
TOK = 192
D = 2048
W = 128
CAP = 18
CAPP = 24
NZ, NX, NY, NC = 4 * 2, 4, 8, 2
NSP = NZ * NX
NTP = NY * NC
ROWS = NSP * CAP
PROWS = NSP * CAPP
HALF = ROWS // 2
OWN = TOK // NTP
OWNP = 16
SP = ("z", "x")
TP = ("y", "c")
ALL = ("z", "x", "y", "c")
MESH_ID = pl.DeviceIdType.MESH
F32 = jnp.float32
BF16 = jnp.bfloat16
FAR_FIRST = (4, 3, 5, 2, 6, 1, 7, 0)

theta_base = 10000.0
norm_eps = 1e-06
very_low = -1e30
RATE_A = 1.4426950408889634 * (DA + ROPE) ** (-0.5)
RATE_B = 1.4426950408889634 * (DB + ROPE) ** (-0.5)


def fdot(a, b):
    return jnp.dot(a, b, preferred_element_type=F32)


def rcopy(src, dst, ssem, rsem, dev):
    return pltpu.make_async_remote_copy(
        src_ref=src, dst_ref=dst, send_sem=ssem, recv_sem=rsem, device_id=dev, device_id_type=MESH_ID
    )


def iota(shape, dim):
    return lax.broadcasted_iota(jnp.int32, shape, dim)


def onehot(cond):
    return jnp.where(cond, 1.0, 0.0).astype(BF16)


def lanes(index, width):
    return pl.ds(pl.multiple_of(index * width, 128), width)


def nt(a, b):
    return lax.dot_general(a, b, (((1,), (1,)), ((), ())), preferred_element_type=F32)


def layer_kernel(
    qa, qb, lat, rope, cosine, sine, kua, kub, vua, vub,
    resid, gain, routes_t, rw_t,
    oa_h, ob_h, sg_h, su_h, sd_h, eg_h, eu_h, ed_h,
    out,
    lz, q_all, wv_t, m_a, l_a, m_b, l_b, acc_a, acc_b, ps, st, pr, sr, heads, cols8,
    wo, sgu, sd, egu, ed,
    r_s, r_r, own_d, po_d, pi_d, sb_d, rb_d,
    hs, hfull, normed,
    po_s, pi_s, sb_s, rb_s, own_s,
    f_s, f_r, comp, expd, g, hacc,
    own_i, po_i, pi_i, isb, irb, j_r, l_s, l_r,
    z_ss, z_rs, zf_ss, zf_rs, zo_ss, zo_rs, q_ss, q_rs, x_ss, x_rs, t_ss, t_rs,
    w_sem, r_ss, r_rs, pd_ss, pd_rs, d_ss, d_rs, e_ss, e_rs, ef_ss, ef_rs,
    ps_ss, ps_rs, s_ss, s_rs, f_ss, f_rs, g_ss, g_rs, gf_ss, gf_rs, go_ss, go_rs,
    pp_ss, pp_rs, i_ss, i_rs, j_ss, j_rs, l_ss, l_rs,
):
    z, x, y, c = (lax.axis_index(a) for a in ALL)
    t = y * NC + c
    sp = z * NX + x
    oc = 1 - c
    partner = (z, x, y, oc)

    def ydev(yy):
        return (z, x, yy, c)

    def tdev(tt):
        return (z, x, tt // NC, lax.rem(tt, NC))

    def sdev(ss):
        return (ss // NX, lax.rem(ss, NX), y, c)

    def xdev(xx):
        return (z, xx, y, c)

    def zdev(zz):
        return (zz, x, y, c)

    def yoff(off):
        return lax.rem(y + off, NY)

    class Ring:
        def __init__(self, pos, dev, win, sems):
            self.pos, self.dev, self.win = pos, dev, win
            self.ss, self.rs, self.fs, self.fr, self.os, self.orr = sems

        def src(self, d, k):
            return lax.rem(self.pos + 8 - k, 8) if d == 0 else lax.rem(self.pos + k, 8)

        def to(self, d):
            return self.dev(self.src(1 - d, 1))

        def ok(self, k, d, h):
            return k < 4 or h == d

        def send(self, d, k, h):
            win = self.win(self.src(d, k - 1), h, c)
            return rcopy(win, win, self.ss.at[d, k - 1, h], self.rs.at[d, k - 1, h], self.to(d))

        def got(self, d, k, h):
            win = self.win(self.src(d, k), h, c)
            return rcopy(win, win, self.ss.at[d, k - 1, h], self.rs.at[d, k - 1, h], self.to(d))

        def fwd(self, d, k, h, core):
            win = self.win(self.src(d, k), h, core)
            return rcopy(win, win, self.fs.at[d, k - 1, h], self.fr.at[d, k - 1, h], partner)

        def own(self, h, core):
            win = self.win(self.pos, h, core)
            return rcopy(win, win, self.os.at[h], self.orr.at[h], partner)

        def run(self, use, own_too, before_use):
            for h in range(2):
                for d in range(2):
                    self.send(d, 1, h).start()
                if own_too:
                    self.own(h, c).start()
            for k in range(1, 5):
                for h in range(2):
                    for d in range(2):
                        if self.ok(k, d, h):
                            self.got(d, k, h).wait_recv()
                            if self.ok(k + 1, d, h) and k < 4:
                                self.send(d, k + 1, h).start()
                            self.fwd(d, k, h, c).start()
                if k == 1:
                    before_use()
                    if own_too:
                        for h in range(2):
                            self.own(h, oc).wait_recv()
                    use(self.pos, True)
                else:
                    for d in range(2):
                        for h in range(2):
                            self.fwd(d, k - 1, h, oc).wait_recv()
                        use(self.src(d, k - 1), False)
            self.fwd(0, 4, 0, oc).wait_recv()
            self.fwd(1, 4, 1, oc).wait_recv()
            use(self.src(0, 4), False)

        def finish(self, own_too):
            for h in range(2):
                if own_too:
                    self.own(h, c).wait_send()
                for k in range(1, 5):
                    for d in range(2):
                        if self.ok(k, d, h):
                            self.send(d, k, h).wait_send()
                            self.fwd(d, k, h, c).wait_send()

    weights = [
        (ob_h, wo.at[0:VB]), (oa_h, wo.at[VB:VB + VA]), (sg_h, sgu.at[:, 0:W]), (su_h, sgu.at[:, W:2 * W]), (sd_h, sd),
        (eg_h, egu.at[:, 0:W]), (eu_h, egu.at[:, W:2 * W]), (ed_h, ed),
    ]
    loads = [pltpu.make_async_copy(a, b, w_sem.at[i]) for i, (a, b) in enumerate(weights)]
    for load in loads:
        load.start()

    barrier = pltpu.get_barrier_semaphore()

    def greet_t(k, _):
        pl.semaphore_signal(barrier, inc=1, device_id=tdev(lax.rem(t + k, NTP)), device_id_type=MESH_ID)
        return 0

    def greet_s(k, _):
        pl.semaphore_signal(barrier, inc=1, device_id=sdev(lax.rem(sp + k, NSP)), device_id_type=MESH_ID)
        return 0

    lax.fori_loop(1, NTP, greet_t, 0)
    lax.fori_loop(1, NSP, greet_s, 0)

    def turn(value):
        wide = value.astype(F32)
        swapped = jnp.concatenate([wide[:, ROPE // 2:], wide[:, 0:ROPE // 2]], axis=1)
        return wide * cosine[...] + swapped * sine[...]

    rot = turn(rope[...])
    lz[z, :, 0:512] = lat[...]
    lz[z, :, 512:640] = jnp.concatenate([jnp.zeros((TOK, 64), F32), rot, rot], axis=1).astype(BF16)
    wide_a, wide_b = qa[...], qb[...]
    q_all[x] = jnp.concatenate(
        [
            wide_b[:, 0:DB].astype(F32),
            wide_a[:, 0:DA].astype(F32),
            turn(wide_a[:, DA:DA + ROPE]),
            turn(wide_b[:, DB:DB + ROPE]),
        ],
        axis=1,
    ).astype(BF16)
    wv_t[0:VB] = nt(onehot(iota((VB, VB), 0) == iota((VB, VB), 1)), vub[...]).astype(BF16)
    wv_t[VB:VB + VA] = nt(onehot(iota((VA, VA), 0) == iota((VA, VA), 1)), vua[...]).astype(BF16)

    names_t = onehot((iota((128, TOK), 0) == routes_t[0:1, :]) | (iota((128, TOK), 0) == routes_t[1:2, :]))
    upper = onehot(iota((TOK, TOK), 0) < iota((TOK, TOK), 1))
    before_t = fdot(names_t, upper)

    def slot_row(k):
        rank = jnp.sum(jnp.where(iota((128, TOK), 0) == routes_t[k:k + 1, :], before_t, 0.0), axis=0, keepdims=True)
        return routes_t[k:k + 1, :] * CAPP + rank.astype(jnp.int32)

    r_s[...] = jnp.zeros_like(r_s)
    r_s[0:OWN, :] = resid[...]

    i_col = iota((ROWS, 1), 0)
    comp[...] = onehot(iota((ROWS, PROWS), 1) == i_col + (CAPP - CAP) * ((i_col * 3641) >> 16))
    j_col = iota((PROWS, 1), 0)
    j_q = (j_col * 2731) >> 16
    j_r0 = j_col - CAPP * j_q
    expd[...] = onehot(iota((PROWS, ROWS), 1) == jnp.where(j_r0 < CAP, CAP * j_q + j_r0, -1))

    pl.semaphore_wait(barrier, NTP - 1 + NSP - 1)

    def resid_copy(k, to):
        tt = lax.rem(t + k, NTP) if to else lax.rem(t + NTP - k, NTP)
        return rcopy(r_s.at[:, lanes(tt if to else t, W)], r_r.at[t if to else tt], r_ss.at[k], r_rs.at[k], tdev(tt))

    def resid_send(k, _):
        resid_copy(k, True).start()
        return 0

    r_r[t] = r_s[:, lanes(t, W)]

    def pair_out(value, off, own, po, pi, ss, rs):
        left, right = value[:, 0:W], value[:, W:2 * W]
        own[off] = jnp.where(c == 0, left, right)
        po[off] = jnp.where(c == 0, right, left).astype(BF16)
        rcopy(po.at[off], pi.at[off], ss.at[off], rs.at[off], partner).start()

    def pair_wait(off, po, pi, ss, rs):
        rcopy(po.at[off], pi.at[off], ss.at[off], rs.at[off], partner).wait()

    def y_copy(off, sb, rb, ss, rs):
        return rcopy(sb.at[off], rb.at[off], ss.at[off], rs.at[off], ydev(yoff(off)))

    def scatter_start(cols, own, po, pi, sb, rb, pss, prs, ss, rs, lead=3):
        for n in range(NY + lead):
            if n < NY:
                off = FAR_FIRST[n]
                pair_out(cols(yoff(off)), off, own, po, pi, pss, prs)
            if n >= lead:
                off = FAR_FIRST[n - lead]
                pair_wait(off, po, pi, pss, prs)
                if off:
                    sb[off] = (own[off] + pi[off].astype(F32)).astype(BF16)
                    y_copy(off, sb, rb, ss, rs).start()

    def scatter_end(own, pi, sb, rb, ss, rs):
        total = own[0] + pi[0].astype(F32)
        for off in range(1, NY):
            y_copy(off, sb, rb, ss, rs).wait()
            total = total + rb[off].astype(F32)
        return total

    def z_win(zz, h, core):
        start = pl.multiple_of(core * (TOK // 2) + h * (TOK // 4), TOK // 4)
        return lz.at[zz, pl.ds(start, TOK // 4), :]

    def q_copy(off, to):
        src = x if to else lax.rem(x + NX - off, NX)
        return rcopy(q_all.at[src], q_all.at[src], q_ss.at[off], q_rs.at[off], xdev(lax.rem(x + off, NX)))

    def queries_here():
        lax.fori_loop(1, NTP, resid_send, 0)
        for off in (2, 1, 3):
            q_copy(off, False).wait_recv()

    def block(zz, first):
        rows = lz[zz]
        part, twice = rows[:, 0:512], rows[:, 512:640].astype(F32)
        lane = iota((TOK, 128), 1)
        keys_b = fdot(part, kub[...])
        keys_a = jnp.concatenate([fdot(part, kua[...]), twice[:, 64:128]], axis=1)
        keys_a = jnp.where(lane < 96, keys_a, 0.0).astype(BF16)
        keys_b = jnp.concatenate([keys_b, jnp.where(lane < 96, 0.0, twice)], axis=1).astype(BF16)
        values = nt(wv_t[...], part).astype(BF16)
        queries = q_all[...].reshape(NX * TOK, 256)
        if first:
            shape = (TOK, NX * TOK)
            seen = x * TOK + iota(shape, 0) <= iota(shape, 1)
        for scores, rate, m, l, acc, lo, hi in (
            (nt(keys_b, queries), RATE_B, m_b, l_b, acc_b, 0, VB),
            (nt(keys_a, queries[:, 128:256]), RATE_A, m_a, l_a, acc_a, VB, VB + VA),
        ):
            if first:
                scores = jnp.where(seen, scores, very_low)
                top = jnp.max(scores, axis=0, keepdims=True)
                expo = jnp.where(seen, jnp.exp2((scores - top) * rate), 0.0)
                l[...] = jnp.sum(expo, axis=0, keepdims=True)
                acc[...] = fdot(values[lo:hi], expo.astype(BF16))
            else:
                top = jnp.maximum(m[...], jnp.max(scores, axis=0, keepdims=True))
                expo = jnp.exp2((scores - top) * rate)
                fade = jnp.exp2((m[...] - top) * rate)
                l[...] = l[...] * fade + jnp.sum(expo, axis=0, keepdims=True)
                acc[...] = acc[...] * fade + fdot(values[lo:hi], expo.astype(BF16))
            m[...] = top

    def use_block(zz, first):
        if first:
            block(zz, True)
        else:
            pl.when(zz < z)(lambda: block(zz, False))

    z_ring = Ring(z, zdev, z_win, (z_ss, z_rs, zf_ss, zf_rs, zo_ss, zo_rs))
    for off in (2, 1, 3):
        q_copy(off, True).start()
    z_ring.run(use_block, False, queries_here)

    share_b = jnp.where(l_b[...] > 0, 1.0 / l_b[...], 0.0)
    share_a = jnp.where(l_a[...] > 0, 1.0 / l_a[...], 0.0)
    out_b, out_a = (acc_b[...] * share_b).astype(BF16), (acc_a[...] * share_a).astype(BF16)
    for xx in range(NX):
        cut = slice(xx * TOK, (xx + 1) * TOK)
        ps[xx, 0:VB] = out_b[:, cut]
        ps[xx, VB:VB + VA] = out_a[:, cut]
        for i, stat in enumerate((m_b, l_b, m_a, l_a)):
            st[xx, i:i + 1, :] = stat[:, cut]
            st[xx, i + 4:i + 5, :] = stat[:, cut]

    def x_copy(src, dst, ss, rs, off, to):
        there = lax.rem(x + off, NX) if to else lax.rem(x + NX - off, NX)
        return rcopy(src.at[there], dst.at[x if to else there], ss.at[off], rs.at[off], xdev(there))

    for off in (2, 1, 3):
        x_copy(st, sr, t_ss, t_rs, off, True).start()
        x_copy(ps, pr, x_ss, x_rs, off, True).start()
    pr[x] = ps[x]
    sr[x] = st[x]
    for load in loads[:2]:
        load.wait()
    for off in range(1, NX):
        x_copy(st, sr, t_ss, t_rs, off, False).wait()
        x_copy(ps, pr, x_ss, x_rs, off, False).wait()
    merged = []
    for row, rate, lo, hi in ((0, RATE_B, 0, VB), (2, RATE_A, VB, VB + VA)):
        tops = [sr[i, row:row + 1, :] for i in range(NX)]
        top = functools.reduce(jnp.maximum, tops)
        part = [jnp.exp2((tops[i] - top) * rate) * sr[i, row + 1:row + 2, :] for i in range(NX)]
        whole = 1.0 / sum(part)
        merged.append(sum(pr[i, lo:hi].astype(F32) * (part[i] * whole) for i in range(NX)))
    turned = jnp.concatenate(merged, axis=0).astype(BF16)
    heads[...] = nt(onehot(iota((TOK, TOK), 0) == iota((TOK, TOK), 1)), turned).astype(BF16)

    def head_cols(yy):
        return fdot(heads[...], wo[:, lanes(yy, 2 * W)])

    scatter_start(head_cols, own_d, po_d, pi_d, sb_d, rb_d, pd_ss, pd_rs, d_ss, d_rs)

    def resid_wait(k, _):
        resid_copy(k, False).wait()
        return 0

    mixed = scatter_end(own_d, pi_d, sb_d, rb_d, d_ss, d_rs)
    lax.fori_loop(1, NTP, resid_wait, 0)
    i12 = iota((TOK, 1), 0)
    pick12 = onehot(iota((TOK, NTP * OWNP), 1) == i12 + (OWNP - OWN) * ((i12 * 5462) >> 16))
    resid_cols = fdot(pick12, r_r[...].reshape(NTP * OWNP, W))
    hs[...] = (resid_cols + mixed).astype(BF16)

    hfull[:, lanes(t, W)] = hs[...]

    def e_copy(off):
        return rcopy(hs, hfull.at[:, lanes(t, W)], e_ss.at[off], e_rs.at[off], ydev(yoff(off)))

    def e_got(off):
        src = lanes(lax.rem(y + NY - off, NY) * NC + c, W)
        return rcopy(hs, hfull.at[:, src], e_ss.at[off], e_rs.at[off], ydev(yoff(off)))

    def e_fwd(off, core):
        win = hfull.at[:, lanes(lax.rem(y + NY - off, NY) * NC + core, W)]
        return rcopy(win, win, ef_ss.at[off], ef_rs.at[off], partner)

    for off in FAR_FIRST[:-1]:
        e_copy(off).start()
    e_fwd(0, c).start()
    for off in (1, 7, 2, 6, 3, 5, 4):
        e_got(off).wait_recv()
        e_fwd(off, c).start()
    for off in range(NY):
        e_fwd(off, oc).wait_recv()

    def norm_rows(b, _):
        rows = pl.ds(pl.multiple_of(b * 16, 16), 16)
        wide = hfull[rows, :].astype(F32)
        mean = jnp.mean(wide * wide, axis=-1, keepdims=True)
        normed[rows, :] = (wide * lax.rsqrt(mean + norm_eps) * gain[...]).astype(BF16)
        return 0

    lax.fori_loop(0, TOK // 16, norm_rows, 0)

    place = onehot((iota((PROWS, TOK), 0) == slot_row(0)) | (iota((PROWS, TOK), 0) == slot_row(1)))
    f_s[...] = fdot(place, normed[:, lanes(t, W)]).reshape(NSP, CAPP, W).astype(BF16)
    f_r[sp] = f_s[sp]

    def sp_copy(k, src, dst, ss, rs, to):
        peer = lax.rem(sp + k, NSP) if to else lax.rem(sp + NSP - k, NSP)
        return rcopy(src.at[peer], dst.at[sp if to else peer], ss.at[k], rs.at[k], sdev(peer))

    def f_send(k, _):
        sp_copy(k, f_s, f_r, f_ss, f_rs, True).start()
        return 0

    def f_wait(k, _):
        sp_copy(k, f_s, f_r, f_ss, f_rs, False).wait()
        return 0

    lax.fori_loop(1, NSP, f_send, 0)

    for load in loads[2:]:
        load.wait()
    both = fdot(normed[...], sgu[...])
    gate, up = both[:, 0:W], both[:, W:2 * W]
    shared_act = (gate / (1.0 + jnp.exp(-gate)) * up).astype(BF16)

    def shared_cols(yy):
        return fdot(shared_act, sd[:, lanes(yy, 2 * W)])

    scatter_start(shared_cols, own_s, po_s, pi_s, sb_s, rb_s, ps_ss, ps_rs, s_ss, s_rs)

    lax.fori_loop(1, NSP, f_wait, 0)
    g[y, :, lanes(c, W)] = fdot(comp[...], f_r[...].astype(F32).reshape(PROWS, W).astype(BF16)).astype(BF16)

    def g_win(yy, h, core):
        return g.at[yy, pl.ds(h * HALF, HALF), lanes(core, W)]

    def gate_up(yy, first):
        value = fdot(g[yy], egu[pl.ds(pl.multiple_of(yy * 2 * W, 2 * W), 2 * W), :])
        hacc[...] = value if first else hacc[...] + value

    y_ring = Ring(y, ydev, g_win, (g_ss, g_rs, gf_ss, gf_rs, go_ss, go_rs))
    y_ring.run(gate_up, True, lambda: None)
    gate, up = hacc[:, 0:W], hacc[:, W:2 * W]
    act = (gate / (1.0 + jnp.exp(-gate)) * up).astype(BF16)

    def i_pair(off):
        pair_out(fdot(act, ed[:, lanes(yoff(off), 2 * W)]), off, own_i, po_i, pi_i, pp_ss, pp_rs)

    def i_copy(d, k, h):
        return rcopy(isb.at[d, k - 1, h], irb.at[d, k - 1, h], i_ss.at[d, k - 1, h], i_rs.at[d, k - 1, h], y_ring.to(d))

    def i_step(k):
        for h in range(2):
            for d in range(2):
                if k > 1 or h == d:
                    off = (5 - k) if d == 0 else (3 + k)
                    rows = pl.ds(h * HALF, HALF)
                    total = own_i[off, rows, :] + pi_i[off, rows, :].astype(F32)
                    if k > 2 or (k == 2 and h == d):
                        i_copy(d, k - 1, h).wait_recv()
                        total = total + irb[d, k - 2, h].astype(F32)
                    isb[d, k - 1, h] = total.astype(BF16)
                    i_copy(d, k, h).start()

    i_pair(4)
    i_pair(3)
    i_pair(5)
    pair_wait(4, po_i, pi_i, pp_ss, pp_rs)
    i_step(1)
    i_pair(2)
    i_pair(6)
    pair_wait(3, po_i, pi_i, pp_ss, pp_rs)
    pair_wait(5, po_i, pi_i, pp_ss, pp_rs)
    i_step(2)
    i_pair(1)
    i_pair(7)
    i_pair(0)
    pair_wait(2, po_i, pi_i, pp_ss, pp_rs)
    pair_wait(6, po_i, pi_i, pp_ss, pp_rs)
    i_step(3)
    pair_wait(1, po_i, pi_i, pp_ss, pp_rs)
    pair_wait(7, po_i, pi_i, pp_ss, pp_rs)
    i_step(4)
    pair_wait(0, po_i, pi_i, pp_ss, pp_rs)
    for h in range(2):
        rows = pl.ds(h * HALF, HALF)
        total = own_i[0, rows, :] + pi_i[0, rows, :].astype(F32)
        for d in range(2):
            i_copy(d, 4, h).wait_recv()
            total = total + irb[d, 3, h].astype(F32)
        own_i[0, rows, :] = total

    f_s[...] = fdot(expd[...], own_i[0].astype(BF16)).reshape(NSP, CAPP, W).astype(BF16)
    j_r[sp] = f_s[sp]

    def j_send(k, _):
        sp_copy(k, f_s, j_r, j_ss, j_rs, True).start()
        return 0

    def j_wait(k, _):
        sp_copy(k, f_s, j_r, j_ss, j_rs, False).wait()
        return 0

    lax.fori_loop(1, NSP, j_send, 0)
    rows8 = jnp.concatenate(
        [slot_row(0).astype(F32), slot_row(1).astype(F32), rw_t[0:1, :], rw_t[1:2, :], jnp.zeros((4, TOK), F32)], axis=0
    )
    cols8[...] = jnp.transpose(rows8)
    final = hs[...].astype(F32) + scatter_end(own_s, pi_s, sb_s, rb_s, s_ss, s_rs)
    lax.fori_loop(1, NSP, j_wait, 0)
    back = j_r[...].astype(F32).reshape(PROWS, W).astype(BF16)
    for k in range(2):
        pick = onehot(iota((TOK, PROWS), 1) == cols8[:, k:k + 1].astype(jnp.int32))
        final = final + fdot(pick, back) * cols8[:, k + 2:k + 3]

    j16 = iota((NTP * OWNP, 1), 0)
    spread = onehot(iota((NTP * OWNP, TOK), 1) == jnp.where((j16 & 15) < OWN, OWN * (j16 >> 4) + (j16 & 15), -1))
    l_s[...] = fdot(spread, final.astype(BF16)).astype(BF16).reshape(NTP, OWNP, W)
    l_r[:, lanes(t, W)] = l_s[t]

    def l_copy(k, to):
        tt = lax.rem(t + k, NTP) if to else lax.rem(t + NTP - k, NTP)
        return rcopy(l_s.at[tt], l_r.at[:, lanes(t if to else tt, W)], l_ss.at[k], l_rs.at[k], tdev(tt))

    def l_send(k, _):
        l_copy(k, True).start()
        return 0

    def l_wait(k, _):
        l_copy(k, False).wait()
        return 0

    lax.fori_loop(1, NTP, l_send, 0)
    for off in range(1, NY):
        e_copy(off).wait_send()
    for off in range(NY):
        e_fwd(off, c).wait_send()
    z_ring.finish(False)
    y_ring.finish(True)
    for off in range(1, NX):
        q_copy(off, True).wait_send()
    for k in range(1, 5):
        for h in range(2):
            for d in range(2):
                if k > 1 or h == d:
                    i_copy(d, k, h).wait_send()
    lax.fori_loop(1, NTP, l_wait, 0)
    out[...] = l_r[0:OWN, :]


def layer(vmem_args, hbm_args):
    dma = pltpu.SemaphoreType.DMA
    vm = pltpu.VMEM
    row = vm((1, NX * TOK), F32)
    scratch = [
        vm((NZ, TOK, 640), BF16), vm((NX, TOK, 256), BF16), vm((VA + VB, 512), BF16), row, row, row, row,
        vm((VA, NX * TOK), F32), vm((VB, NX * TOK), F32), vm((NX, VA + VB, TOK), BF16), vm((NX, 8, TOK), F32),
        vm((NX, VA + VB, TOK), BF16), vm((NX, 8, TOK), F32), vm((TOK, VA + VB), BF16), vm((TOK, 8), F32),
        vm((VA + VB, D), BF16), vm((D, 2 * W), BF16), vm((W, D), BF16), vm((D, 2 * W), BF16), vm((W, D), BF16),
        vm((OWNP, D), BF16), vm((NTP, OWNP, W), BF16),
        vm((NY, TOK, W), F32), vm((NY, TOK, W), BF16), vm((NY, TOK, W), BF16), vm((NY, TOK, W), BF16), vm((NY, TOK, W), BF16),
        vm((TOK, W), BF16), vm((TOK, D), BF16), vm((TOK, D), BF16),
        vm((NY, TOK, W), BF16), vm((NY, TOK, W), BF16), vm((NY, TOK, W), BF16), vm((NY, TOK, W), BF16), vm((NY, TOK, W), F32),
        vm((NSP, CAPP, W), BF16), vm((NSP, CAPP, W), BF16), vm((ROWS, PROWS), BF16), vm((PROWS, ROWS), BF16), vm((NY, ROWS, 2 * W), BF16), vm((ROWS, 2 * W), F32),
        vm((NY, ROWS, W), F32), vm((NY, ROWS, W), BF16), vm((NY, ROWS, W), BF16), vm((2, 4, 2, HALF, W), BF16), vm((2, 4, 2, HALF, W), BF16),
        vm((NSP, CAPP, W), BF16), vm((NTP, OWNP, W), BF16), vm((OWNP, D), BF16),
    ] + [
        dma(n) for n in (
            (2, 4, 2), (2, 4, 2), (2, 4, 2), (2, 4, 2), (2,), (2,), (NX,), (NX,), (NX,), (NX,), (NX,), (NX,),
            (8,), (NTP,), (NTP,), (NY,), (NY,), (NY,), (NY,), (NY,), (NY,), (NY,), (NY,),
            (NY,), (NY,), (NY,), (NY,), (NSP,), (NSP,),
            (2, 4, 2), (2, 4, 2), (2, 4, 2), (2, 4, 2), (2,), (2,),
            (NY,), (NY,), (2, 4, 2), (2, 4, 2), (NSP,), (NSP,), (NTP,), (NTP,),
        )
    ]
    vspec = pl.BlockSpec(memory_space=pltpu.VMEM)
    hspec = pl.BlockSpec(memory_space=pl.ANY)
    return pl.pallas_call(
        layer_kernel,
        out_shape=jax.ShapeDtypeStruct((OWN, D), BF16),
        in_specs=[vspec] * len(vmem_args) + [hspec] * len(hbm_args),
        out_specs=vspec,
        scratch_shapes=scratch,
        compiler_params=pltpu.CompilerParams(collective_id=1, has_side_effects=True, vmem_limit_bytes=60 * 2**20),
        name="layer",
    )(*vmem_args, *hbm_args)


def tables(positions):
    freqs = theta_base ** (-(2.0 * jnp.arange(ROPE // 2, dtype=F32)) / ROPE)
    angles = positions.astype(F32)[:, None] * freqs[None, :]
    cosine, sine = jnp.cos(angles), jnp.sin(angles)
    return jnp.concatenate([cosine, cosine], axis=1), jnp.concatenate([-sine, sine], axis=1)


def shards(
    residual, query_a, query_b, latents, rope_key, key_up_a, value_up_a, key_up_b, value_up_b,
    out_proj_a, out_proj_b, norm_gain, routes, route_weights, shared_gate, shared_up, shared_down,
    expert_gate, expert_up, expert_down,
):
    first_row = lax.axis_index(SP) * TOK
    cosine, sine = tables(first_row + jnp.arange(TOK, dtype=jnp.int32))
    return layer(
        (
            query_a, query_b, latents, rope_key, cosine, sine, key_up_a, key_up_b, value_up_a, value_up_b,
            residual, norm_gain.reshape(1, D), routes.T, route_weights.T,
        ),
        (out_proj_a, out_proj_b, shared_gate, shared_up, shared_down, expert_gate[0], expert_up[0], expert_down[0]),
    )


def solution(mesh):
    torus = Mesh(mesh.devices.reshape(NZ, NX, NY, NC), ALL)
    rows, cols, split = P(SP, None), P(None, TP), P(TP, None)
    in_specs = (
        P(SP + TP, None), P(SP, TP), P(SP, TP), rows, rows, cols, cols, cols, cols, split, split, P(), rows, rows,
        cols, cols, split, P(SP, None, TP), P(SP, None, TP), P(SP, TP, None),
    )
    return jax.shard_map(
        shards, mesh=torus, in_specs=in_specs, out_specs=P(SP + TP, None), check_vma=False
    )
```

```python
import functools

import jax
import jax.numpy as jnp
from jax import lax
from jax.experimental import pallas as pl
from jax.experimental.pallas import tpu as pltpu
from jax.sharding import Mesh
from jax.sharding import PartitionSpec as P

DA = 64
VA = 64
DB = 128
VB = 128
ROPE = 32
TOK = 192
D = 2048
W = 128
CAP = 18
CAPP = 24
NZ, NX, NY, NC = 4 * 2, 4, 8, 2
NSP = NZ * NX
NTP = NY * NC
ROWS = NSP * CAP
PROWS = NSP * CAPP
Z_PIECES = 2
PIECES = 4
PIECE = ROWS // PIECES
OWN = TOK // NTP
OWNP = 16
SP = ("z", "x")
TP = ("y", "c")
ALL = ("z", "x", "y", "c")
MESH_ID = pl.DeviceIdType.MESH
F32 = jnp.float32
BF16 = jnp.bfloat16
FAR_FIRST = (4, 3, 5, 2, 6, 1, 7, 0)

theta_base = 10000.0
norm_eps = 1e-06
very_low = -1e30
RATE_A = 1.4426950408889634 * (DA + ROPE) ** (-0.5)
RATE_B = 1.4426950408889634 * (DB + ROPE) ** (-0.5)


def fdot(a, b):
    return jnp.dot(a, b, preferred_element_type=F32)


def rcopy(src, dst, ssem, rsem, dev):
    return pltpu.make_async_remote_copy(
        src_ref=src, dst_ref=dst, send_sem=ssem, recv_sem=rsem, device_id=dev, device_id_type=MESH_ID
    )


def iota(shape, dim):
    return lax.broadcasted_iota(jnp.int32, shape, dim)


def onehot(cond):
    return jnp.where(cond, 1.0, 0.0).astype(BF16)


def lanes(index, width):
    return pl.ds(pl.multiple_of(index * width, 128), width)


def nt(a, b):
    return lax.dot_general(a, b, (((1,), (1,)), ((), ())), preferred_element_type=F32)


def layer_kernel(
    qa, qb_t, lat, rope_t, cosine, sine, kua_t, kub, vua_t, vub,
    resid, gain, routes_t, rw_t,
    oa_h, ob_h, sg_h, su_h, sd_h, eg_h, eu_h, ed_h,
    out,
    lz, q_all, wv_t, m_a, l_a, m_b, l_b, acc_a, acc_b, ps, st, pr, sr, heads, cols8,
    wo, sgu, sd, egu, ed,
    r_s, r_r, own_d, po_d, pi_d, sb_d, rb_d,
    hs, hidden,
    po_s, pi_s, sb_s, rb_s, own_s,
    f_s, f_r, tight, ssq, g, hacc,
    own_i, po_i, pi_i, isb, irb, j_r, l_s, l_r,
    z_ss, z_rs, zf_ss, zf_rs, zo_ss, zo_rs, q_ss, q_rs, x_ss, x_rs, t_ss, t_rs,
    w_sem, r_ss, r_rs, pd_ss, pd_rs, d_ss, d_rs, e_ss, e_rs, ef_ss, ef_rs,
    ps_ss, ps_rs, s_ss, s_rs, f_ss, f_rs, g_ss, g_rs, gf_ss, gf_rs, go_ss, go_rs,
    pp_ss, pp_rs, i_ss, i_rs, j_ss, j_rs, l_ss, l_rs,
):
    z, x, y, c = (lax.axis_index(a) for a in ALL)
    t = y * NC + c
    sp = z * NX + x
    oc = 1 - c
    partner = (z, x, y, oc)

    def ydev(yy):
        return (z, x, yy, c)

    def tdev(tt):
        return (z, x, tt // NC, lax.rem(tt, NC))

    def sdev(ss):
        return (ss // NX, lax.rem(ss, NX), y, c)

    def xdev(xx):
        return (z, xx, y, c)

    def zdev(zz):
        return (zz, x, y, c)

    def yoff(off):
        return lax.rem(y + off, NY)

    class Ring:
        def __init__(self, pos, dev, win, pieces, sems):
            self.pos, self.dev, self.win, self.pieces = pos, dev, win, pieces
            self.ss, self.rs, self.fs, self.fr, self.os, self.orr = sems

        def src(self, d, k):
            return lax.rem(self.pos + 8 - k, 8) if d == 0 else lax.rem(self.pos + k, 8)

        def to(self, d):
            return self.dev(self.src(1 - d, 1))

        def ok(self, k, d, h):
            return k < 4 or (k == 4 and (h < self.pieces // 2) == (d == 0))

        def send(self, d, k, h):
            win = self.win(self.src(d, k - 1), h, c)
            return rcopy(win, win, self.ss.at[d, k - 1, h], self.rs.at[d, k - 1, h], self.to(d))

        def got(self, d, k, h):
            win = self.win(self.src(d, k), h, c)
            return rcopy(win, win, self.ss.at[d, k - 1, h], self.rs.at[d, k - 1, h], self.to(d))

        def fwd(self, d, k, h, core):
            win = self.win(self.src(d, k), h, core)
            return rcopy(win, win, self.fs.at[d, k - 1, h], self.fr.at[d, k - 1, h], partner)

        def own(self, h, core):
            win = self.win(self.pos, h, core)
            return rcopy(win, win, self.os.at[h], self.orr.at[h], partner)

        def pass_on(self, k, d, h):
            if self.ok(k, d, h):
                self.got(d, k, h).wait_recv()
                if self.ok(k + 1, d, h):
                    self.send(d, k + 1, h).start()
                self.fwd(d, k, h, c).start()

        def whole(self, d, k):
            for h in range(self.pieces):
                if self.ok(k, d, h):
                    self.fwd(d, k, h, oc).wait_recv()

        def run(self, use, own_too, after_start, before_use):
            half = self.pieces // 2
            for h in range(self.pieces):
                for d in range(2):
                    self.send(d, 1, h).start()
                if own_too:
                    self.own(h, c).start()
            after_start()
            for k in range(1, 5):
                for h in range(self.pieces):
                    for d in range(2):
                        self.pass_on(k, d, h)
                    if k > 1 and h == half - 1:
                        self.whole(0, k - 1)
                        use(self.src(0, k - 1), False)
                if k > 1:
                    self.whole(1, k - 1)
                    use(self.src(1, k - 1), False)
                else:
                    before_use()
                    if own_too:
                        for h in range(self.pieces):
                            self.own(h, oc).wait_recv()
                    use(self.pos, True)
            self.whole(0, 4)
            self.whole(1, 4)
            use(self.src(0, 4), False)

        def finish(self, own_too):
            for h in range(self.pieces):
                if own_too:
                    self.own(h, c).wait_send()
                for k in range(1, 5):
                    for d in range(2):
                        if self.ok(k, d, h):
                            self.send(d, k, h).wait_send()
                            self.fwd(d, k, h, c).wait_send()

    weights = [
        (ob_h, wo.at[0:VB]), (oa_h, wo.at[VB:VB + VA]), (sg_h, sgu.at[:, 0:W]), (su_h, sgu.at[:, W:2 * W]), (sd_h, sd),
        (eg_h, egu.at[:, 0:W]), (eu_h, egu.at[:, W:2 * W]), (ed_h, ed),
    ]
    loads = [pltpu.make_async_copy(a, b, w_sem.at[i]) for i, (a, b) in enumerate(weights)]
    for load in loads:
        load.start()

    barrier = pltpu.get_barrier_semaphore()

    def greet_t(k, _):
        pl.semaphore_signal(barrier, inc=1, device_id=tdev(lax.rem(t + k, NTP)), device_id_type=MESH_ID)
        return 0

    def greet_s(k, _):
        pl.semaphore_signal(barrier, inc=1, device_id=sdev(lax.rem(sp + k, NSP)), device_id_type=MESH_ID)
        return 0

    lax.fori_loop(1, NTP, greet_t, 0)
    lax.fori_loop(1, NSP, greet_s, 0)

    def unit(size):
        return onehot(iota((size, size), 0) == iota((size, size), 1))

    def turn(value):
        wide = value.astype(F32)
        swapped = jnp.concatenate([wide[ROPE // 2:], wide[0:ROPE // 2]], axis=0)
        return (wide * cosine[...] + swapped * sine[...]).astype(BF16)

    unit_tok = unit(TOK)
    rot = turn(rope_t[...])
    lz[z, :, 0:512] = lat[...]
    lz[z, :, 512:640] = nt(unit_tok, jnp.concatenate([jnp.zeros((64, TOK), BF16), rot, rot], axis=0)).astype(BF16)
    qa_t = nt(unit(DA + ROPE), qa[...]).astype(BF16)
    q_t = jnp.concatenate([qb_t[0:DB], qa_t[0:DA], turn(qa_t[DA:DA + ROPE]), turn(qb_t[DB:DB + ROPE])], axis=0)
    q_all[x] = nt(unit_tok, q_t).astype(BF16)
    wv_t[0:VB] = nt(unit(VB), vub[...]).astype(BF16)
    wv_t[VB:VB + VA] = vua_t[...]

    names_t = onehot((iota((128, TOK), 0) == routes_t[0:1, :]) | (iota((128, TOK), 0) == routes_t[1:2, :]))
    upper = onehot(iota((TOK, TOK), 0) < iota((TOK, TOK), 1))
    before_t = fdot(names_t, upper)

    def slot_row(k):
        rank = jnp.sum(jnp.where(iota((128, TOK), 0) == routes_t[k:k + 1, :], before_t, 0.0), axis=0, keepdims=True)
        return routes_t[k:k + 1, :] * CAPP + rank.astype(jnp.int32)

    r_s[...] = jnp.zeros_like(r_s)
    tight[ROWS:, :] = jnp.zeros((8, W), F32)
    r_s[0:OWN, :] = resid[...]

    pl.semaphore_wait(barrier, NTP - 1 + NSP - 1)

    def resid_copy(k, to):
        tt = lax.rem(t + k, NTP) if to else lax.rem(t + NTP - k, NTP)
        return rcopy(r_s.at[:, lanes(tt if to else t, W)], r_r.at[t if to else tt], r_ss.at[k], r_rs.at[k], tdev(tt))

    def resid_send(k, _):
        resid_copy(k, True).start()
        return 0

    r_r[t] = r_s[:, lanes(t, W)]

    def pair_out(value, off, own, po, pi, ss, rs):
        left, right = value[:, 0:W], value[:, W:2 * W]
        own[off] = jnp.where(c == 0, left, right)
        po[off] = jnp.where(c == 0, right, left).astype(BF16)
        rcopy(po.at[off], pi.at[off], ss.at[off], rs.at[off], partner).start()

    def pair_wait(off, po, pi, ss, rs):
        rcopy(po.at[off], pi.at[off], ss.at[off], rs.at[off], partner).wait()

    def y_copy(off, sb, rb, ss, rs):
        return rcopy(sb.at[off], rb.at[off], ss.at[off], rs.at[off], ydev(yoff(off)))

    def scatter_start(cols, own, po, pi, sb, rb, pss, prs, ss, rs, lead=3):
        for n in range(NY + lead):
            if n < NY:
                off = FAR_FIRST[n]
                pair_out(cols(yoff(off)), off, own, po, pi, pss, prs)
            if n >= lead:
                off = FAR_FIRST[n - lead]
                pair_wait(off, po, pi, pss, prs)
                if off:
                    sb[off] = (own[off] + pi[off].astype(F32)).astype(BF16)
                    y_copy(off, sb, rb, ss, rs).start()

    def scatter_send(own, po, pi, sb, rb, pss, prs, ss, rs):
        pair_wait(0, po, pi, pss, prs)
        for off in FAR_FIRST[:-1]:
            pair_wait(off, po, pi, pss, prs)
            sb[off] = (own[off] + pi[off].astype(F32)).astype(BF16)
            y_copy(off, sb, rb, ss, rs).start()

    def scatter_end(own, pi, sb, rb, ss, rs):
        total = own[0] + pi[0].astype(F32)
        for off in range(1, NY):
            y_copy(off, sb, rb, ss, rs).wait()
            total = total + rb[off].astype(F32)
        return total

    def z_win(zz, h, core):
        size = TOK // 2 // Z_PIECES
        start = pl.multiple_of(core * (TOK // 2) + h * size, size)
        return lz.at[zz, pl.ds(start, size), :]

    def q_copy(off, to):
        src = x if to else lax.rem(x + NX - off, NX)
        return rcopy(q_all.at[src], q_all.at[src], q_ss.at[off], q_rs.at[off], xdev(lax.rem(x + off, NX)))

    def queries_here():
        lax.fori_loop(1, NTP, resid_send, 0)
        for off in (2, 1, 3):
            q_copy(off, False).wait_recv()

    def block(zz, first):
        rows = lz[zz]
        part, twice = rows[:, 0:512], rows[:, 512:640].astype(F32)
        lane = iota((TOK, 128), 1)
        keys_b = fdot(part, kub[...])
        keys_a = jnp.concatenate([nt(part, kua_t[...]), twice[:, 64:128]], axis=1)
        keys_a = jnp.where(lane < 96, keys_a, 0.0).astype(BF16)
        keys_b = jnp.concatenate([keys_b, jnp.where(lane < 96, 0.0, twice)], axis=1).astype(BF16)
        values = nt(wv_t[...], part).astype(BF16)
        queries = q_all[...].reshape(NX * TOK, 256)
        if first:
            shape = (TOK, NX * TOK)
            seen = x * TOK + iota(shape, 0) <= iota(shape, 1)
        for scores, rate, m, l, acc, lo, hi in (
            (nt(keys_b, queries), RATE_B, m_b, l_b, acc_b, 0, VB),
            (nt(keys_a, queries[:, 128:256]), RATE_A, m_a, l_a, acc_a, VB, VB + VA),
        ):
            if first:
                scores = jnp.where(seen, scores, very_low)
                top = jnp.max(scores, axis=0, keepdims=True)
                expo = jnp.where(seen, jnp.exp2((scores - top) * rate), 0.0)
                l[...] = jnp.sum(expo, axis=0, keepdims=True)
                acc[...] = fdot(values[lo:hi], expo.astype(BF16))
            else:
                top = jnp.maximum(m[...], jnp.max(scores, axis=0, keepdims=True))
                expo = jnp.exp2((scores - top) * rate)
                fade = jnp.exp2((m[...] - top) * rate)
                l[...] = l[...] * fade + jnp.sum(expo, axis=0, keepdims=True)
                acc[...] = acc[...] * fade + fdot(values[lo:hi], expo.astype(BF16))
            m[...] = top

    def use_block(zz, first):
        if first:
            block(zz, True)
        else:
            pl.when(zz < z)(lambda: block(zz, False))

    z_ring = Ring(z, zdev, z_win, Z_PIECES, (z_ss, z_rs, zf_ss, zf_rs, zo_ss, zo_rs))
    for off in (2, 1, 3):
        q_copy(off, True).start()
    z_ring.run(use_block, False, lambda: None, queries_here)

    share_b = jnp.where(l_b[...] > 0, 1.0 / l_b[...], 0.0)
    share_a = jnp.where(l_a[...] > 0, 1.0 / l_a[...], 0.0)
    out_b, out_a = (acc_b[...] * share_b).astype(BF16), (acc_a[...] * share_a).astype(BF16)
    for xx in range(NX):
        cut = slice(xx * TOK, (xx + 1) * TOK)
        ps[xx, 0:VB] = out_b[:, cut]
        ps[xx, VB:VB + VA] = out_a[:, cut]
        for i, stat in enumerate((m_b, l_b, m_a, l_a)):
            st[xx, i:i + 1, :] = stat[:, cut]
            st[xx, i + 4:i + 5, :] = stat[:, cut]

    def x_copy(src, dst, ss, rs, off, to):
        there = lax.rem(x + off, NX) if to else lax.rem(x + NX - off, NX)
        return rcopy(src.at[there], dst.at[x if to else there], ss.at[off], rs.at[off], xdev(there))

    for off in (2, 1, 3):
        x_copy(st, sr, t_ss, t_rs, off, True).start()
        x_copy(ps, pr, x_ss, x_rs, off, True).start()
    pr[x] = ps[x]
    sr[x] = st[x]
    for load in loads:
        load.wait()
    for i in range(NTP):
        cut = slice(i * W, (i + 1) * W)
        column = jnp.transpose(jnp.broadcast_to(gain[:, cut], (8, W)))[:, 0:1]
        for ref in (sgu, egu):
            ref[cut, :] = (ref[cut, :].astype(F32) * column).astype(BF16)
    for off in range(1, NX):
        x_copy(st, sr, t_ss, t_rs, off, False).wait()
        x_copy(ps, pr, x_ss, x_rs, off, False).wait()
    merged = []
    for row, rate, lo, hi in ((0, RATE_B, 0, VB), (2, RATE_A, VB, VB + VA)):
        tops = [sr[i, row:row + 1, :] for i in range(NX)]
        top = functools.reduce(jnp.maximum, tops)
        part = [jnp.exp2((tops[i] - top) * rate) * sr[i, row + 1:row + 2, :] for i in range(NX)]
        whole = 1.0 / sum(part)
        merged.append(sum(pr[i, lo:hi].astype(F32) * (part[i] * whole) for i in range(NX)))
    turned = jnp.concatenate(merged, axis=0).astype(BF16)
    heads[...] = nt(unit_tok, turned).astype(BF16)

    def head_cols(yy):
        return fdot(heads[...], wo[:, lanes(yy, 2 * W)])

    scatter_start(head_cols, own_d, po_d, pi_d, sb_d, rb_d, pd_ss, pd_rs, d_ss, d_rs)

    def resid_wait(k, _):
        resid_copy(k, False).wait()
        return 0

    mixed = scatter_end(own_d, pi_d, sb_d, rb_d, d_ss, d_rs)
    lax.fori_loop(1, NTP, resid_wait, 0)
    i12 = iota((TOK, 1), 0)
    pick12 = onehot(iota((TOK, NTP * OWNP), 1) == i12 + (OWNP - OWN) * ((i12 * 5462) >> 16))
    resid_cols = fdot(pick12, r_r[...].reshape(NTP * OWNP, W))
    hs[...] = (resid_cols + mixed).astype(BF16)

    place = onehot((iota((PROWS, TOK), 0) == slot_row(0)) | (iota((PROWS, TOK), 0) == slot_row(1)))

    f_s[...] = fdot(place, hs[...]).reshape(NSP, CAPP, W).astype(BF16)
    f_r[sp] = f_s[sp]

    def sp_copy(k, src, dst, ss, rs, to):
        peer = lax.rem(sp + k, NSP) if to else lax.rem(sp + NSP - k, NSP)
        return rcopy(src.at[peer], dst.at[sp if to else peer], ss.at[k], rs.at[k], sdev(peer))

    def f_send(k, _):
        sp_copy(k, f_s, f_r, f_ss, f_rs, True).start()
        return 0

    def f_wait(k, _):
        sp_copy(k, f_s, f_r, f_ss, f_rs, False).wait()
        return 0

    lax.fori_loop(1, NSP, f_send, 0)

    hidden[:, lanes(t, W)] = hs[...]

    def e_copy(off):
        return rcopy(hs, hidden.at[:, lanes(t, W)], e_ss.at[off], e_rs.at[off], ydev(yoff(off)))

    def e_got(off):
        src = lanes(lax.rem(y + NY - off, NY) * NC + c, W)
        return rcopy(hs, hidden.at[:, src], e_ss.at[off], e_rs.at[off], ydev(yoff(off)))

    def e_fwd(off, core):
        win = hidden.at[:, lanes(lax.rem(y + NY - off, NY) * NC + core, W)]
        return rcopy(win, win, ef_ss.at[off], ef_rs.at[off], partner)

    for off in FAR_FIRST[:-1]:
        e_copy(off).start()
    e_fwd(0, c).start()
    lax.fori_loop(1, NSP, f_wait, 0)
    for e in range(NSP):
        tight[e * CAP:e * CAP + CAPP, :] = f_r[e].astype(F32)
    g[y, :, lanes(c, W)] = tight[0:ROWS, :].astype(BF16)

    def g_win(yy, h, core):
        return g.at[yy, pl.ds(h * PIECE, PIECE), lanes(core, W)]

    def gate_up(yy, first):
        wide = g[yy].astype(F32)
        wide = wide * wide
        squares = wide[:, 0:W] + wide[:, W:2 * W]
        ssq[...] = squares if first else ssq[...] + squares
        value = fdot(g[yy], egu[pl.ds(pl.multiple_of(yy * 2 * W, 2 * W), 2 * W), :])
        hacc[...] = value if first else hacc[...] + value

    y_ring = Ring(y, ydev, g_win, PIECES, (g_ss, g_rs, gf_ss, gf_rs, go_ss, go_rs))
    def hidden_relay():
        for off in (1, 7, 2, 6, 3, 5, 4):
            e_got(off).wait_recv()
            e_fwd(off, c).start()

    def root(total):
        return lax.rsqrt(jnp.sum(total, axis=1, keepdims=True) * (1.0 / D) + norm_eps)

    def gated(both, scale):
        gate, up = both[:, 0:W] * scale, both[:, W:2 * W] * scale
        return (gate / (1.0 + jnp.exp(-gate)) * up).astype(BF16)

    def shared_pairs():
        for off in range(NY):
            e_fwd(off, oc).wait_recv()
        total = jnp.zeros((TOK, W), F32)
        for i in range(NTP):
            wide = hidden[:, i * W:(i + 1) * W].astype(F32)
            total = total + wide * wide
        shared_act = gated(fdot(hidden[...], sgu[...]), root(total))
        for off in range(NY):
            value = fdot(shared_act, sd[:, lanes(yoff(off), 2 * W)])
            pair_out(value, off, own_s, po_s, pi_s, ps_ss, ps_rs)

    y_ring.run(gate_up, True, hidden_relay, shared_pairs)
    act = gated(hacc[...], root(ssq[...]))

    def i_pair(off):
        pair_out(fdot(act, ed[:, lanes(yoff(off), 2 * W)]), off, own_i, po_i, pi_i, pp_ss, pp_rs)

    def i_copy(d, k, h):
        return rcopy(isb.at[d, k - 1, h], irb.at[d, k - 1, h], i_ss.at[d, k - 1, h], i_rs.at[d, k - 1, h], y_ring.to(d))

    def i_ok(d, k, h):
        return k > 1 or (h < PIECES // 2) == (d == 0)

    def i_step(k):
        for h in range(PIECES):
            for d in range(2):
                if i_ok(d, k, h):
                    off = (5 - k) if d == 0 else (3 + k)
                    rows = pl.ds(h * PIECE, PIECE)
                    total = own_i[off, rows, :] + pi_i[off, rows, :].astype(F32)
                    if k > 1 and i_ok(d, k - 1, h):
                        i_copy(d, k - 1, h).wait_recv()
                        total = total + irb[d, k - 2, h].astype(F32)
                    isb[d, k - 1, h] = total.astype(BF16)
                    i_copy(d, k, h).start()

    i_pair(4)
    i_pair(3)
    i_pair(5)
    pair_wait(4, po_i, pi_i, pp_ss, pp_rs)
    i_step(1)
    i_pair(2)
    i_pair(6)
    pair_wait(3, po_i, pi_i, pp_ss, pp_rs)
    pair_wait(5, po_i, pi_i, pp_ss, pp_rs)
    i_step(2)
    i_pair(1)
    i_pair(7)
    i_pair(0)
    pair_wait(2, po_i, pi_i, pp_ss, pp_rs)
    pair_wait(6, po_i, pi_i, pp_ss, pp_rs)
    i_step(3)
    pair_wait(1, po_i, pi_i, pp_ss, pp_rs)
    pair_wait(7, po_i, pi_i, pp_ss, pp_rs)
    i_step(4)
    pair_wait(0, po_i, pi_i, pp_ss, pp_rs)
    for h in range(PIECES):
        rows = pl.ds(h * PIECE, PIECE)
        total = own_i[0, rows, :] + pi_i[0, rows, :].astype(F32)
        for d in range(2):
            i_copy(d, 4, h).wait_recv()
            total = total + irb[d, 3, h].astype(F32)
        tight[rows, :] = total

    for e in range(NSP):
        f_s[e] = tight[e * CAP:e * CAP + CAPP, :].astype(BF16)
    j_r[sp] = f_s[sp]

    def j_send(k, _):
        sp_copy(k, f_s, j_r, j_ss, j_rs, True).start()
        return 0

    def j_wait(k, _):
        sp_copy(k, f_s, j_r, j_ss, j_rs, False).wait()
        return 0

    lax.fori_loop(1, NSP, j_send, 0)
    scatter_send(own_s, po_s, pi_s, sb_s, rb_s, ps_ss, ps_rs, s_ss, s_rs)
    rows8 = jnp.concatenate(
        [slot_row(0).astype(F32), slot_row(1).astype(F32), rw_t[0:1, :], rw_t[1:2, :], jnp.zeros((4, TOK), F32)], axis=0
    )
    cols8[...] = jnp.transpose(rows8)
    final = hs[...].astype(F32) + scatter_end(own_s, pi_s, sb_s, rb_s, s_ss, s_rs)
    lax.fori_loop(1, NSP, j_wait, 0)
    back = j_r[...].astype(F32).reshape(PROWS, W).astype(BF16)
    for k in range(2):
        pick = onehot(iota((TOK, PROWS), 1) == cols8[:, k:k + 1].astype(jnp.int32))
        final = final + fdot(pick, back) * cols8[:, k + 2:k + 3]

    j16 = iota((NTP * OWNP, 1), 0)
    spread = onehot(iota((NTP * OWNP, TOK), 1) == jnp.where((j16 & 15) < OWN, OWN * (j16 >> 4) + (j16 & 15), -1))
    l_s[...] = fdot(spread, final.astype(BF16)).astype(BF16).reshape(NTP, OWNP, W)
    l_r[:, lanes(t, W)] = l_s[t]

    def l_copy(k, to):
        tt = lax.rem(t + k, NTP) if to else lax.rem(t + NTP - k, NTP)
        return rcopy(l_s.at[tt], l_r.at[:, lanes(t if to else tt, W)], l_ss.at[k], l_rs.at[k], tdev(tt))

    def l_send(k, _):
        l_copy(k, True).start()
        return 0

    def l_wait(k, _):
        l_copy(k, False).wait()
        return 0

    lax.fori_loop(1, NTP, l_send, 0)
    for off in range(1, NY):
        e_copy(off).wait_send()
    for off in range(NY):
        e_fwd(off, c).wait_send()
    z_ring.finish(False)
    y_ring.finish(True)
    for off in range(1, NX):
        q_copy(off, True).wait_send()
    for k in range(1, 5):
        for h in range(PIECES):
            for d in range(2):
                if i_ok(d, k, h):
                    i_copy(d, k, h).wait_send()
    lax.fori_loop(1, NTP, l_wait, 0)
    out[...] = l_r[0:OWN, :]


def layer(vmem_args, hbm_args):
    dma = pltpu.SemaphoreType.DMA
    vm = pltpu.VMEM
    row = vm((1, NX * TOK), F32)
    zsem, ysem = (2, 4, Z_PIECES), (2, 4, PIECES)
    scratch = [
        vm((NZ, TOK, 640), BF16), vm((NX, TOK, 256), BF16), vm((VA + VB, 512), BF16), row, row, row, row,
        vm((VA, NX * TOK), F32), vm((VB, NX * TOK), F32), vm((NX, VA + VB, TOK), BF16), vm((NX, 8, TOK), F32),
        vm((NX, VA + VB, TOK), BF16), vm((NX, 8, TOK), F32), vm((TOK, VA + VB), BF16), vm((TOK, 8), F32),
        vm((VA + VB, D), BF16), vm((D, 2 * W), BF16), vm((W, D), BF16), vm((D, 2 * W), BF16), vm((W, D), BF16),
        vm((OWNP, D), BF16), vm((NTP, OWNP, W), BF16),
        vm((NY, TOK, W), F32), vm((NY, TOK, W), BF16), vm((NY, TOK, W), BF16), vm((NY, TOK, W), BF16), vm((NY, TOK, W), BF16),
        vm((TOK, W), BF16), vm((TOK, D), BF16),
        vm((NY, TOK, W), BF16), vm((NY, TOK, W), BF16), vm((NY, TOK, W), BF16), vm((NY, TOK, W), BF16), vm((NY, TOK, W), F32),
        vm((NSP, CAPP, W), BF16), vm((NSP, CAPP, W), BF16), vm((ROWS + 8, W), F32), vm((ROWS, W), F32), vm((NY, ROWS, 2 * W), BF16), vm((ROWS, 2 * W), F32),
        vm((NY, ROWS, W), F32), vm((NY, ROWS, W), BF16), vm((NY, ROWS, W), BF16), vm((2, 4, PIECES, PIECE, W), BF16), vm((2, 4, PIECES, PIECE, W), BF16),
        vm((NSP, CAPP, W), BF16), vm((NTP, OWNP, W), BF16), vm((OWNP, D), BF16),
    ] + [
        dma(n) for n in (
            zsem, zsem, zsem, zsem, (2,), (2,), (NX,), (NX,), (NX,), (NX,), (NX,), (NX,),
            (8,), (NTP,), (NTP,), (NY,), (NY,), (NY,), (NY,), (NY,), (NY,), (NY,), (NY,),
            (NY,), (NY,), (NY,), (NY,), (NSP,), (NSP,),
            ysem, ysem, ysem, ysem, (PIECES,), (PIECES,),
            (NY,), (NY,), ysem, ysem, (NSP,), (NSP,), (NTP,), (NTP,),
        )
    ]
    vspec = pl.BlockSpec(memory_space=pltpu.VMEM)
    hspec = pl.BlockSpec(memory_space=pl.ANY)
    return pl.pallas_call(
        layer_kernel,
        out_shape=jax.ShapeDtypeStruct((OWN, D), BF16),
        in_specs=[vspec] * len(vmem_args) + [hspec] * len(hbm_args),
        out_specs=vspec,
        scratch_shapes=scratch,
        compiler_params=pltpu.CompilerParams(collective_id=1, has_side_effects=True, vmem_limit_bytes=60 * 2**20),
        name="layer",
    )(*vmem_args, *hbm_args)


def tables(positions):
    freqs = theta_base ** (-(2.0 * jnp.arange(ROPE // 2, dtype=F32)) / ROPE)
    angles = positions.astype(F32)[None, :] * freqs[:, None]
    cosine, sine = jnp.cos(angles), jnp.sin(angles)
    return jnp.concatenate([cosine, cosine], axis=0), jnp.concatenate([-sine, sine], axis=0)


def shards(
    residual, query_a, query_b, latents, rope_key, key_up_a, value_up_a, key_up_b, value_up_b,
    out_proj_a, out_proj_b, norm_gain, routes, route_weights, shared_gate, shared_up, shared_down,
    expert_gate, expert_up, expert_down,
):
    first_row = lax.axis_index(SP) * TOK
    cosine, sine = tables(first_row + jnp.arange(TOK, dtype=jnp.int32))
    return layer(
        (
            query_a, query_b.T, latents, rope_key.T, cosine, sine, key_up_a.T, key_up_b, value_up_a.T, value_up_b,
            residual, norm_gain.reshape(1, D), routes.T, route_weights.T,
        ),
        (out_proj_a, out_proj_b, shared_gate, shared_up, shared_down, expert_gate[0], expert_up[0], expert_down[0]),
    )


def solution(mesh):
    torus = Mesh(mesh.devices.reshape(NZ, NX, NY, NC), ALL)
    rows, cols, split = P(SP, None), P(None, TP), P(TP, None)
    in_specs = (
        P(SP + TP, None), P(SP, TP), P(SP, TP), rows, rows, cols, cols, cols, cols, split, split, P(), rows, rows,
        cols, cols, split, P(SP, None, TP), P(SP, None, TP), P(SP, TP, None),
    )
    return jax.shard_map(
        shards, mesh=torus, in_specs=in_specs, out_specs=P(SP + TP, None), check_vma=False
    )
```

```python
import functools

import jax
import jax.numpy as jnp
from jax import lax
from jax.experimental import pallas as pl
from jax.experimental.pallas import tpu as pltpu
from jax.sharding import Mesh
from jax.sharding import PartitionSpec as P

DA = 64
VA = 64
DB = 128
VB = 128
ROPE = 32
TOK = 192
D = 2048
W = 128
CAP = 18
CAPP = 24
NZ, NX, NY, NC = 4 * 2, 4, 8, 2
NSP = NZ * NX
NTP = NY * NC
ROWS = NSP * CAP
PROWS = NSP * CAPP
Z_PIECES = 2
PIECES = 4
PIECE = ROWS // PIECES
OWN = TOK // NTP
OWNP = 16
SP = ("z", "x")
TP = ("y", "c")
ALL = ("z", "x", "y", "c")
MESH_ID = pl.DeviceIdType.MESH
F32 = jnp.float32
BF16 = jnp.bfloat16
FAR_FIRST = (4, 3, 5, 2, 6, 1, 7, 0)
MERGED = (4, 2, 6, 1, 7, 3, 5, 0)

theta_base = 10000.0
norm_eps = 1e-06
very_low = -1e30
RATE_A = 1.4426950408889634 * (DA + ROPE) ** (-0.5)
RATE_B = 1.4426950408889634 * (DB + ROPE) ** (-0.5)


def fdot(a, b):
    return jnp.dot(a, b, preferred_element_type=F32)


def rcopy(src, dst, ssem, rsem, dev):
    return pltpu.make_async_remote_copy(
        src_ref=src, dst_ref=dst, send_sem=ssem, recv_sem=rsem, device_id=dev, device_id_type=MESH_ID
    )


def iota(shape, dim):
    return lax.broadcasted_iota(jnp.int32, shape, dim)


def onehot(cond):
    return jnp.where(cond, 1.0, 0.0).astype(BF16)


def lanes(index, width):
    return pl.ds(pl.multiple_of(index * width, 128), width)


def nt(a, b):
    return lax.dot_general(a, b, (((1,), (1,)), ((), ())), preferred_element_type=F32)


def layer_kernel(
    qa, qb_t, lat, rope_t, cosine, sine, kua_t, kub, vua_t, vub,
    resid, gain, routes_t, rw_t,
    oa_h, ob_h, sg_h, su_h, sd_h, eg_h, eu_h, ed_h,
    out,
    lz, q_all, wv_t, m_a, l_a, m_b, l_b, acc_a, acc_b, ps, st, pr, sr, heads, cols8,
    wo, sgu, sd, egu, ed,
    r_s, r_r, own_d, po_d, pi_d, sb_d, rb_d,
    hs, hidden,
    po_s, pi_s, sb_s, rb_s, own_s,
    f_s, f_r, tight, ssq, g, hacc,
    own_i, po_i, pi_i, isb, irb, j_r, l_s, l_r,
    f2_s, f2_r, j2_r, l2_s, l2_r, mg_d, mg_s,
    z_ss, z_rs, zf_ss, zf_rs, zo_ss, zo_rs, q_ss, q_rs, x_ss, x_rs, t_ss, t_rs,
    w_sem, r_ss, r_rs, pd_ss, pd_rs, d_ss, d_rs, e_ss, e_rs, ef_ss, ef_rs,
    ps_ss, ps_rs, s_ss, s_rs, f_ss, f_rs, g_ss, g_rs, gf_ss, gf_rs, go_ss, go_rs,
    pp_ss, pp_rs, i_ss, i_rs, j_ss, j_rs, l_ss, l_rs,
    f2_ss, f2_rs, j2_ss, j2_rs, l2_ss, l2_rs, md_ss, md_rs, ms_ss, ms_rs, g4_ss, g4_rs,
):
    z, x, y, c = (lax.axis_index(a) for a in ALL)
    t = y * NC + c
    t4 = lax.rem(y + 4, NY) * NC + c
    sp = z * NX + x
    oc = 1 - c
    partner = (z, x, y, oc)

    def ydev(yy):
        return (z, x, yy, c)

    def tdev(tt):
        return (z, x, tt // NC, lax.rem(tt, NC))

    def sdev(ss):
        return (ss // NX, lax.rem(ss, NX), y, c)

    def xdev(xx):
        return (z, xx, y, c)

    def zdev(zz):
        return (zz, x, y, c)

    def yoff(off):
        return lax.rem(y + off, NY)

    class Ring:
        def __init__(self, pos, dev, win, pieces, sems, short=False):
            self.short = short
            self.pos, self.dev, self.win, self.pieces = pos, dev, win, pieces
            self.ss, self.rs, self.fs, self.fr, self.os, self.orr = sems

        def src(self, d, k):
            return lax.rem(self.pos + 8 - k, 8) if d == 0 else lax.rem(self.pos + k, 8)

        def to(self, d):
            return self.dev(self.src(1 - d, 1))

        def ok(self, k, d, h):
            return k < 4 or (k == 4 and not self.short and (h < self.pieces // 2) == (d == 0))

        def send(self, d, k, h):
            win = self.win(self.src(d, k - 1), h, c)
            return rcopy(win, win, self.ss.at[d, k - 1, h], self.rs.at[d, k - 1, h], self.to(d))

        def got(self, d, k, h):
            win = self.win(self.src(d, k), h, c)
            return rcopy(win, win, self.ss.at[d, k - 1, h], self.rs.at[d, k - 1, h], self.to(d))

        def fwd(self, d, k, h, core):
            win = self.win(self.src(d, k), h, core)
            return rcopy(win, win, self.fs.at[d, k - 1, h], self.fr.at[d, k - 1, h], partner)

        def own(self, h, core):
            win = self.win(self.pos, h, core)
            return rcopy(win, win, self.os.at[h], self.orr.at[h], partner)

        def pass_on(self, k, d, h):
            if self.ok(k, d, h):
                self.got(d, k, h).wait_recv()
                if self.ok(k + 1, d, h):
                    self.send(d, k + 1, h).start()
                self.fwd(d, k, h, c).start()

        def whole(self, d, k):
            for h in range(self.pieces):
                if self.ok(k, d, h):
                    self.fwd(d, k, h, oc).wait_recv()

        def run(self, use, own_too, after_start, before_use, fourth=None, fourth_end=None):
            half = self.pieces // 2
            for h in range(self.pieces):
                for d in range(2):
                    self.send(d, 1, h).start()
                if own_too:
                    self.own(h, c).start()
            after_start()
            for k in range(1, 5):
                if k == 4 and self.short:
                    fourth()
                for h in range(self.pieces):
                    for d in range(2):
                        self.pass_on(k, d, h)
                    if k > 1 and h == half - 1:
                        self.whole(0, k - 1)
                        use(self.src(0, k - 1), False)
                if k > 1:
                    self.whole(1, k - 1)
                    use(self.src(1, k - 1), False)
                else:
                    before_use()
                    if own_too:
                        for h in range(self.pieces):
                            self.own(h, oc).wait_recv()
                    use(self.pos, True)
            if self.short:
                fourth_end()
            else:
                self.whole(0, 4)
                self.whole(1, 4)
            use(self.src(0, 4), False)

        def finish(self, own_too):
            for h in range(self.pieces):
                if own_too:
                    self.own(h, c).wait_send()
                for k in range(1, 5):
                    for d in range(2):
                        if self.ok(k, d, h):
                            self.send(d, k, h).wait_send()
                            self.fwd(d, k, h, c).wait_send()

    weights = [
        (ob_h, wo.at[0:VB]), (oa_h, wo.at[VB:VB + VA]), (sg_h, sgu.at[:, 0:W]), (su_h, sgu.at[:, W:2 * W]), (sd_h, sd),
        (eg_h, egu.at[:, 0:W]), (eu_h, egu.at[:, W:2 * W]), (ed_h, ed),
    ]
    loads = [pltpu.make_async_copy(a, b, w_sem.at[i]) for i, (a, b) in enumerate(weights)]
    for load in loads:
        load.start()

    barrier = pltpu.get_barrier_semaphore()

    def greet_t(k, _):
        pl.semaphore_signal(barrier, inc=1, device_id=tdev(lax.rem(t + k, NTP)), device_id_type=MESH_ID)
        return 0

    def greet_s(k, _):
        pl.semaphore_signal(barrier, inc=1, device_id=sdev(lax.rem(sp + k, NSP)), device_id_type=MESH_ID)
        return 0

    lax.fori_loop(1, NTP, greet_t, 0)
    lax.fori_loop(1, NSP, greet_s, 0)

    def unit(size):
        return onehot(iota((size, size), 0) == iota((size, size), 1))

    def turn(value):
        wide = value.astype(F32)
        swapped = jnp.concatenate([wide[ROPE // 2:], wide[0:ROPE // 2]], axis=0)
        return (wide * cosine[...] + swapped * sine[...]).astype(BF16)

    unit_tok = unit(TOK)
    rot = turn(rope_t[...])
    lz[z, :, 0:512] = lat[...]
    lz[z, :, 512:640] = nt(unit_tok, jnp.concatenate([jnp.zeros((64, TOK), BF16), rot, rot], axis=0)).astype(BF16)
    qa_t = nt(unit(DA + ROPE), qa[...]).astype(BF16)
    q_t = jnp.concatenate([qb_t[0:DB], qa_t[0:DA], turn(qa_t[DA:DA + ROPE]), turn(qb_t[DB:DB + ROPE])], axis=0)
    q_all[x] = nt(unit_tok, q_t).astype(BF16)
    wv_t[0:VB] = nt(unit(VB), vub[...]).astype(BF16)
    wv_t[VB:VB + VA] = vua_t[...]

    names_t = onehot((iota((128, TOK), 0) == routes_t[0:1, :]) | (iota((128, TOK), 0) == routes_t[1:2, :]))
    upper = onehot(iota((TOK, TOK), 0) < iota((TOK, TOK), 1))
    before_t = fdot(names_t, upper)

    def slot_row(k):
        rank = jnp.sum(jnp.where(iota((128, TOK), 0) == routes_t[k:k + 1, :], before_t, 0.0), axis=0, keepdims=True)
        return routes_t[k:k + 1, :] * CAPP + rank.astype(jnp.int32)

    r_s[...] = jnp.zeros_like(r_s)
    tight[ROWS:, :] = jnp.zeros((8, W), F32)
    r_s[0:OWN, :] = resid[...]

    pl.semaphore_wait(barrier, NTP - 1 + NSP - 1)

    def resid_copy(k, to):
        tt = lax.rem(t + k, NTP) if to else lax.rem(t + NTP - k, NTP)
        return rcopy(r_s.at[:, lanes(tt if to else t, W)], r_r.at[t if to else tt], r_ss.at[k], r_rs.at[k], tdev(tt))

    def resid_send(k, _):
        resid_copy(k, True).start()
        return 0

    r_r[t] = r_s[:, lanes(t, W)]

    def pair_out(value, off, own, po, pi, ss, rs):
        left, right = value[:, 0:W], value[:, W:2 * W]
        own[off] = jnp.where(c == 0, left, right)
        po[off] = jnp.where(c == 0, right, left).astype(BF16)
        rcopy(po.at[off], pi.at[off], ss.at[off], rs.at[off], partner).start()

    def pair_wait(off, po, pi, ss, rs):
        rcopy(po.at[off], pi.at[off], ss.at[off], rs.at[off], partner).wait()

    def y_copy(off, sb, rb, ss, rs):
        return rcopy(sb.at[off], rb.at[off], ss.at[off], rs.at[off], ydev(yoff(off)))

    def merge_copy(i, sb, mg, ms, mr):
        half = sb.at[4, pl.ds(i * (TOK // 2), TOK // 2), :]
        return rcopy(half, mg.at[i], ms.at[i], mr.at[i], ydev(yoff(1 if i == 0 else 7)))

    def scatter_one(off, own, po, pi, sb, rb, pss, prs, ss, rs, mg, ms, mr):
        pair_wait(off, po, pi, pss, prs)
        if off == 0:
            return
        total = own[off] + pi[off].astype(F32)
        if off in (3, 5):
            i = 0 if off == 3 else 1
            merge_copy(i, sb, mg, ms, mr).wait()
            came = mg[i].astype(F32)
            still = jnp.zeros_like(came)
            total = total + jnp.concatenate([came, still] if i == 0 else [still, came], axis=0)
        sb[off] = total.astype(BF16)
        if off == 4:
            for i in range(2):
                merge_copy(i, sb, mg, ms, mr).start()
        else:
            y_copy(off, sb, rb, ss, rs).start()

    def scatter_start(cols, own, po, pi, *rest, lead=3):
        for n in range(NY + lead):
            if n < NY:
                off = MERGED[n]
                pair_out(cols(yoff(off)), off, own, po, pi, rest[2], rest[3])
            if n >= lead:
                scatter_one(MERGED[n - lead], own, po, pi, *rest)

    def scatter_send(offs, *all_of):
        for off in offs:
            scatter_one(off, *all_of)

    def scatter_end(own, pi, sb, rb, ss, rs):
        total = own[0] + pi[0].astype(F32)
        for off in (2, 6, 1, 7, 3, 5):
            y_copy(off, sb, rb, ss, rs).wait()
            total = total + rb[off].astype(F32)
        return total

    def z_win(zz, h, core):
        size = TOK // 2 // Z_PIECES
        start = pl.multiple_of(core * (TOK // 2) + h * size, size)
        return lz.at[zz, pl.ds(start, size), :]

    def q_copy(off, to):
        src = x if to else lax.rem(x + NX - off, NX)
        return rcopy(q_all.at[src], q_all.at[src], q_ss.at[off], q_rs.at[off], xdev(lax.rem(x + off, NX)))

    def queries_here():
        lax.fori_loop(1, NTP, resid_send, 0)
        for off in (2, 1, 3):
            q_copy(off, False).wait_recv()

    def block(zz, first):
        rows = lz[zz]
        part, twice = rows[:, 0:512], rows[:, 512:640].astype(F32)
        lane = iota((TOK, 128), 1)
        keys_b = fdot(part, kub[...])
        keys_a = jnp.concatenate([nt(part, kua_t[...]), twice[:, 64:128]], axis=1)
        keys_a = jnp.where(lane < 96, keys_a, 0.0).astype(BF16)
        keys_b = jnp.concatenate([keys_b, jnp.where(lane < 96, 0.0, twice)], axis=1).astype(BF16)
        values = nt(wv_t[...], part).astype(BF16)
        queries = q_all[...].reshape(NX * TOK, 256)
        if first:
            shape = (TOK, NX * TOK)
            seen = x * TOK + iota(shape, 0) <= iota(shape, 1)
        for scores, rate, m, l, acc, lo, hi in (
            (nt(keys_b, queries), RATE_B, m_b, l_b, acc_b, 0, VB),
            (nt(keys_a, queries[:, 128:256]), RATE_A, m_a, l_a, acc_a, VB, VB + VA),
        ):
            if first:
                scores = jnp.where(seen, scores, very_low)
                top = jnp.max(scores, axis=0, keepdims=True)
                expo = jnp.where(seen, jnp.exp2((scores - top) * rate), 0.0)
                l[...] = jnp.sum(expo, axis=0, keepdims=True)
                acc[...] = fdot(values[lo:hi], expo.astype(BF16))
            else:
                top = jnp.maximum(m[...], jnp.max(scores, axis=0, keepdims=True))
                expo = jnp.exp2((scores - top) * rate)
                fade = jnp.exp2((m[...] - top) * rate)
                l[...] = l[...] * fade + jnp.sum(expo, axis=0, keepdims=True)
                acc[...] = acc[...] * fade + fdot(values[lo:hi], expo.astype(BF16))
            m[...] = top

    def use_block(zz, first):
        if first:
            block(zz, True)
        else:
            pl.when(zz < z)(lambda: block(zz, False))

    z_ring = Ring(z, zdev, z_win, Z_PIECES, (z_ss, z_rs, zf_ss, zf_rs, zo_ss, zo_rs))
    for off in (2, 1, 3):
        q_copy(off, True).start()
    z_ring.run(use_block, False, lambda: None, queries_here)

    share_b = jnp.where(l_b[...] > 0, 1.0 / l_b[...], 0.0)
    share_a = jnp.where(l_a[...] > 0, 1.0 / l_a[...], 0.0)
    out_b, out_a = (acc_b[...] * share_b).astype(BF16), (acc_a[...] * share_a).astype(BF16)
    for xx in range(NX):
        cut = slice(xx * TOK, (xx + 1) * TOK)
        ps[xx, 0:VB] = out_b[:, cut]
        ps[xx, VB:VB + VA] = out_a[:, cut]
        for i, stat in enumerate((m_b, l_b, m_a, l_a)):
            st[xx, i:i + 1, :] = stat[:, cut]
            st[xx, i + 4:i + 5, :] = stat[:, cut]

    def x_copy(src, dst, ss, rs, off, to):
        there = lax.rem(x + off, NX) if to else lax.rem(x + NX - off, NX)
        return rcopy(src.at[there], dst.at[x if to else there], ss.at[off], rs.at[off], xdev(there))

    for off in (2, 1, 3):
        x_copy(st, sr, t_ss, t_rs, off, True).start()
        x_copy(ps, pr, x_ss, x_rs, off, True).start()
    pr[x] = ps[x]
    sr[x] = st[x]
    for load in loads:
        load.wait()
    for i in range(NTP):
        cut = slice(i * W, (i + 1) * W)
        column = jnp.transpose(jnp.broadcast_to(gain[:, cut], (8, W)))[:, 0:1]
        for ref in (sgu, egu):
            ref[cut, :] = (ref[cut, :].astype(F32) * column).astype(BF16)
    for off in range(1, NX):
        x_copy(st, sr, t_ss, t_rs, off, False).wait()
        x_copy(ps, pr, x_ss, x_rs, off, False).wait()
    merged = []
    for row, rate, lo, hi in ((0, RATE_B, 0, VB), (2, RATE_A, VB, VB + VA)):
        tops = [sr[i, row:row + 1, :] for i in range(NX)]
        top = functools.reduce(jnp.maximum, tops)
        part = [jnp.exp2((tops[i] - top) * rate) * sr[i, row + 1:row + 2, :] for i in range(NX)]
        whole = 1.0 / sum(part)
        merged.append(sum(pr[i, lo:hi].astype(F32) * (part[i] * whole) for i in range(NX)))
    turned = jnp.concatenate(merged, axis=0).astype(BF16)
    heads[...] = nt(unit_tok, turned).astype(BF16)

    def head_cols(yy):
        return fdot(heads[...], wo[:, lanes(yy, 2 * W)])

    scatter_start(head_cols, own_d, po_d, pi_d, sb_d, rb_d, pd_ss, pd_rs, d_ss, d_rs, mg_d, md_ss, md_rs)

    def resid_wait(k, _):
        resid_copy(k, False).wait()
        return 0

    mixed = scatter_end(own_d, pi_d, sb_d, rb_d, d_ss, d_rs)
    lax.fori_loop(1, NTP, resid_wait, 0)
    i12 = iota((TOK, 1), 0)
    pick12 = onehot(iota((TOK, NTP * OWNP), 1) == i12 + (OWNP - OWN) * ((i12 * 5462) >> 16))
    resid_cols = fdot(pick12, r_r[...].reshape(NTP * OWNP, W))
    hs[...] = (resid_cols + mixed).astype(BF16)

    place = onehot((iota((PROWS, TOK), 0) == slot_row(0)) | (iota((PROWS, TOK), 0) == slot_row(1)))

    f_s[...] = fdot(place, hs[...]).reshape(NSP, CAPP, W).astype(BF16)
    f_r[sp] = f_s[sp]

    def sp_copy(k, src, dst, ss, rs, to):
        peer = lax.rem(sp + k, NSP) if to else lax.rem(sp + NSP - k, NSP)
        return rcopy(src.at[peer], dst.at[sp if to else peer], ss.at[k], rs.at[k], sdev(peer))

    def f_send(k, _):
        sp_copy(k, f_s, f_r, f_ss, f_rs, True).start()
        return 0

    def f_wait(k, _):
        sp_copy(k, f_s, f_r, f_ss, f_rs, False).wait()
        return 0

    lax.fori_loop(1, NSP, f_send, 0)

    hidden[:, lanes(t, W)] = hs[...]

    def e_copy(off):
        return rcopy(hs, hidden.at[:, lanes(t, W)], e_ss.at[off], e_rs.at[off], ydev(yoff(off)))

    def e_got(off):
        src = lanes(lax.rem(y + NY - off, NY) * NC + c, W)
        return rcopy(hs, hidden.at[:, src], e_ss.at[off], e_rs.at[off], ydev(yoff(off)))

    def e_fwd(off, core):
        win = hidden.at[:, lanes(lax.rem(y + NY - off, NY) * NC + core, W)]
        return rcopy(win, win, ef_ss.at[off], ef_rs.at[off], partner)

    for off in FAR_FIRST[:-1]:
        e_copy(off).start()
    e_fwd(0, c).start()

    def f2_send(k, _):
        sp_copy(k, f2_s, f2_r, f2_ss, f2_rs, True).start()
        return 0

    def f2_wait(k, _):
        sp_copy(k, f2_s, f2_r, f2_ss, f2_rs, False).wait()
        return 0

    lax.fori_loop(1, NSP, f_wait, 0)
    for e in range(NSP):
        tight[e * CAP:e * CAP + CAPP, :] = f_r[e].astype(F32)
    g[y, :, lanes(c, W)] = tight[0:ROWS, :].astype(BF16)

    def g_win(yy, h, core):
        return g.at[yy, pl.ds(h * PIECE, PIECE), lanes(core, W)]

    def gate_up(yy, first):
        wide = g[yy].astype(F32)
        wide = wide * wide
        squares = wide[:, 0:W] + wide[:, W:2 * W]
        ssq[...] = squares if first else ssq[...] + squares
        value = fdot(g[yy], egu[pl.ds(pl.multiple_of(yy * 2 * W, 2 * W), 2 * W), :])
        hacc[...] = value if first else hacc[...] + value

    y_ring = Ring(y, ydev, g_win, PIECES, (g_ss, g_rs, gf_ss, gf_rs, go_ss, go_rs), True)
    def hidden_relay():
        e_got(4).wait_recv()
        f2_s[...] = fdot(place, hidden[:, lanes(t4, W)]).reshape(NSP, CAPP, W).astype(BF16)
        f2_r[sp] = f2_s[sp]
        lax.fori_loop(1, NSP, f2_send, 0)
        e_fwd(4, c).start()
        for off in (1, 7, 2, 6, 3, 5):
            e_got(off).wait_recv()
            e_fwd(off, c).start()

    def root(total):
        return lax.rsqrt(jnp.sum(total, axis=1, keepdims=True) * (1.0 / D) + norm_eps)

    def gated(both, scale):
        gate, up = both[:, 0:W] * scale, both[:, W:2 * W] * scale
        return (gate / (1.0 + jnp.exp(-gate)) * up).astype(BF16)

    def shared_pairs():
        for off in range(NY):
            e_fwd(off, oc).wait_recv()
        total = jnp.zeros((TOK, W), F32)
        for i in range(NTP):
            wide = hidden[:, i * W:(i + 1) * W].astype(F32)
            total = total + wide * wide
        shared_act = gated(fdot(hidden[...], sgu[...]), root(total))
        for off in range(NY):
            value = fdot(shared_act, sd[:, lanes(yoff(off), 2 * W)])
            pair_out(value, off, own_s, po_s, pi_s, ps_ss, ps_rs)

    def g_four(core):
        win = g.at[yoff(4), :, lanes(core, W)]
        return rcopy(win, win, g4_ss, g4_rs, partner)

    def fourth():
        lax.fori_loop(1, NSP, f2_wait, 0)
        for e in range(NSP):
            tight[e * CAP:e * CAP + CAPP, :] = f2_r[e].astype(F32)
        g[yoff(4), :, lanes(c, W)] = tight[0:ROWS, :].astype(BF16)
        g_four(c).start()
        scatter_send((4, 2, 6), own_s, po_s, pi_s, sb_s, rb_s, ps_ss, ps_rs, s_ss, s_rs, mg_s, ms_ss, ms_rs)

    y_ring.run(gate_up, True, hidden_relay, shared_pairs, fourth, lambda: g_four(oc).wait_recv())
    act = gated(hacc[...], root(ssq[...]))

    def i_pair(off):
        pair_out(fdot(act, ed[:, lanes(yoff(off), 2 * W)]), off, own_i, po_i, pi_i, pp_ss, pp_rs)

    def i_copy(d, k, h):
        return rcopy(isb.at[d, k - 1, h], irb.at[d, k - 1, h], i_ss.at[d, k - 1, h], i_rs.at[d, k - 1, h], y_ring.to(d))

    def i_step(k):
        for h in range(PIECES):
            for d in range(2):
                off = (4 - k) if d == 0 else (4 + k)
                rows = pl.ds(h * PIECE, PIECE)
                total = own_i[off, rows, :] + pi_i[off, rows, :].astype(F32)
                if k > 1:
                    i_copy(d, k - 1, h).wait_recv()
                    total = total + irb[d, k - 2, h].astype(F32)
                isb[d, k - 1, h] = total.astype(BF16)
                i_copy(d, k, h).start()

    def i_wait(*offs):
        for off in offs:
            pair_wait(off, po_i, pi_i, pp_ss, pp_rs)

    i_pair(3)
    i_pair(5)
    i_pair(4)
    i_pair(2)
    i_wait(3, 5)
    i_step(1)
    i_pair(6)
    i_wait(4)
    tight[0:ROWS, :] = own_i[4] + pi_i[4].astype(F32)
    for e in range(NSP):
        f2_s[e] = tight[e * CAP:e * CAP + CAPP, :].astype(BF16)
    j2_r[sp] = f2_s[sp]

    def j2_send(k, _):
        sp_copy(k, f2_s, j2_r, j2_ss, j2_rs, True).start()
        return 0

    def j2_wait(k, _):
        sp_copy(k, f2_s, j2_r, j2_ss, j2_rs, False).wait()
        return 0

    lax.fori_loop(1, NSP, j2_send, 0)
    i_wait(2, 6)
    i_step(2)
    i_pair(1)
    i_pair(7)
    i_pair(0)
    i_wait(1, 7)
    i_step(3)
    i_wait(0)
    for h in range(PIECES):
        rows = pl.ds(h * PIECE, PIECE)
        total = own_i[0, rows, :] + pi_i[0, rows, :].astype(F32)
        for d in range(2):
            i_copy(d, 3, h).wait_recv()
            total = total + irb[d, 2, h].astype(F32)
        tight[rows, :] = total

    for e in range(NSP):
        f_s[e] = tight[e * CAP:e * CAP + CAPP, :].astype(BF16)
    j_r[sp] = f_s[sp]

    def j_send(k, _):
        sp_copy(k, f_s, j_r, j_ss, j_rs, True).start()
        return 0

    def j_wait(k, _):
        sp_copy(k, f_s, j_r, j_ss, j_rs, False).wait()
        return 0

    lax.fori_loop(1, NSP, j_send, 0)
    scatter_send((3, 5, 1, 7, 0), own_s, po_s, pi_s, sb_s, rb_s, ps_ss, ps_rs, s_ss, s_rs, mg_s, ms_ss, ms_rs)
    rows8 = jnp.concatenate(
        [slot_row(0).astype(F32), slot_row(1).astype(F32), rw_t[0:1, :], rw_t[1:2, :], jnp.zeros((4, TOK), F32)], axis=0
    )
    cols8[...] = jnp.transpose(rows8)
    j16 = iota((NTP * OWNP, 1), 0)
    spread = onehot(iota((NTP * OWNP, TOK), 1) == jnp.where((j16 & 15) < OWN, OWN * (j16 >> 4) + (j16 & 15), -1))
    picks = [onehot(iota((TOK, PROWS), 1) == cols8[:, k:k + 1].astype(jnp.int32)) for k in range(2)]

    def routed(ref):
        back = ref[...].astype(F32).reshape(PROWS, W).astype(BF16)
        return sum(fdot(picks[k], back) * cols8[:, k + 2:k + 3] for k in range(2))

    def to_rows(value, l_s, l_r, window, ss, rs):
        l_s[...] = fdot(spread, value.astype(BF16)).astype(BF16).reshape(NTP, OWNP, W)
        l_r[:, lanes(window(t), W)] = l_s[t]

        def l_send(k, _):
            l_copy(k, True, l_s, l_r, window, ss, rs).start()
            return 0

        lax.fori_loop(1, NTP, l_send, 0)

    def l_copy(k, to, l_s, l_r, window, ss, rs):
        tt = lax.rem(t + k, NTP) if to else lax.rem(t + NTP - k, NTP)
        return rcopy(l_s.at[tt], l_r.at[:, lanes(window(t if to else tt), W)], ss.at[k], rs.at[k], tdev(tt))

    def near(tt):
        return tt

    def far(tt):
        return lax.rem(tt + NTP // 2, NTP)

    lax.fori_loop(1, NSP, j2_wait, 0)
    to_rows(routed(j2_r), l2_s, l2_r, far, l2_ss, l2_rs)
    final = hs[...].astype(F32) + scatter_end(own_s, pi_s, sb_s, rb_s, s_ss, s_rs)
    lax.fori_loop(1, NSP, j_wait, 0)
    to_rows(final + routed(j_r), l_s, l_r, near, l_ss, l_rs)

    def l_wait(k, _):
        l_copy(k, False, l2_s, l2_r, far, l2_ss, l2_rs).wait()
        l_copy(k, False, l_s, l_r, near, l_ss, l_rs).wait()
        return 0

    for off in range(1, NY):
        e_copy(off).wait_send()
    for off in range(NY):
        e_fwd(off, c).wait_send()
    z_ring.finish(False)
    g_four(c).wait_send()
    y_ring.finish(True)
    for off in range(1, NX):
        q_copy(off, True).wait_send()
    for k in range(1, 4):
        for h in range(PIECES):
            for d in range(2):
                i_copy(d, k, h).wait_send()
    lax.fori_loop(1, NTP, l_wait, 0)
    out[...] = (l_r[0:OWN, :].astype(F32) + l2_r[0:OWN, :].astype(F32)).astype(BF16)


def layer(vmem_args, hbm_args):
    dma = pltpu.SemaphoreType.DMA
    vm = pltpu.VMEM
    row = vm((1, NX * TOK), F32)
    zsem, ysem = (2, 4, Z_PIECES), (2, 4, PIECES)
    scratch = [
        vm((NZ, TOK, 640), BF16), vm((NX, TOK, 256), BF16), vm((VA + VB, 512), BF16), row, row, row, row,
        vm((VA, NX * TOK), F32), vm((VB, NX * TOK), F32), vm((NX, VA + VB, TOK), BF16), vm((NX, 8, TOK), F32),
        vm((NX, VA + VB, TOK), BF16), vm((NX, 8, TOK), F32), vm((TOK, VA + VB), BF16), vm((TOK, 8), F32),
        vm((VA + VB, D), BF16), vm((D, 2 * W), BF16), vm((W, D), BF16), vm((D, 2 * W), BF16), vm((W, D), BF16),
        vm((OWNP, D), BF16), vm((NTP, OWNP, W), BF16),
        vm((NY, TOK, W), F32), vm((NY, TOK, W), BF16), vm((NY, TOK, W), BF16), vm((NY, TOK, W), BF16), vm((NY, TOK, W), BF16),
        vm((TOK, W), BF16), vm((TOK, D), BF16),
        vm((NY, TOK, W), BF16), vm((NY, TOK, W), BF16), vm((NY, TOK, W), BF16), vm((NY, TOK, W), BF16), vm((NY, TOK, W), F32),
        vm((NSP, CAPP, W), BF16), vm((NSP, CAPP, W), BF16), vm((ROWS + 8, W), F32), vm((ROWS, W), F32), vm((NY, ROWS, 2 * W), BF16), vm((ROWS, 2 * W), F32),
        vm((NY, ROWS, W), F32), vm((NY, ROWS, W), BF16), vm((NY, ROWS, W), BF16), vm((2, 4, PIECES, PIECE, W), BF16), vm((2, 4, PIECES, PIECE, W), BF16),
        vm((NSP, CAPP, W), BF16), vm((NTP, OWNP, W), BF16), vm((OWNP, D), BF16),
        vm((NSP, CAPP, W), BF16), vm((NSP, CAPP, W), BF16), vm((NSP, CAPP, W), BF16), vm((NTP, OWNP, W), BF16), vm((OWNP, D), BF16),
        vm((2, TOK // 2, W), BF16), vm((2, TOK // 2, W), BF16),
    ] + [
        dma(n) for n in (
            zsem, zsem, zsem, zsem, (2,), (2,), (NX,), (NX,), (NX,), (NX,), (NX,), (NX,),
            (8,), (NTP,), (NTP,), (NY,), (NY,), (NY,), (NY,), (NY,), (NY,), (NY,), (NY,),
            (NY,), (NY,), (NY,), (NY,), (NSP,), (NSP,),
            ysem, ysem, ysem, ysem, (PIECES,), (PIECES,),
            (NY,), (NY,), ysem, ysem, (NSP,), (NSP,), (NTP,), (NTP,),
            (NSP,), (NSP,), (NSP,), (NSP,), (NTP,), (NTP,), (2,), (2,), (2,), (2,),
        )
    ] + [dma, dma]
    vspec = pl.BlockSpec(memory_space=pltpu.VMEM)
    hspec = pl.BlockSpec(memory_space=pl.ANY)
    return pl.pallas_call(
        layer_kernel,
        out_shape=jax.ShapeDtypeStruct((OWN, D), BF16),
        in_specs=[vspec] * len(vmem_args) + [hspec] * len(hbm_args),
        out_specs=vspec,
        scratch_shapes=scratch,
        compiler_params=pltpu.CompilerParams(collective_id=1, has_side_effects=True, vmem_limit_bytes=60 * 2**20),
        name="layer",
    )(*vmem_args, *hbm_args)


def tables(positions):
    freqs = theta_base ** (-(2.0 * jnp.arange(ROPE // 2, dtype=F32)) / ROPE)
    angles = positions.astype(F32)[None, :] * freqs[:, None]
    cosine, sine = jnp.cos(angles), jnp.sin(angles)
    return jnp.concatenate([cosine, cosine], axis=0), jnp.concatenate([-sine, sine], axis=0)


def shards(
    residual, query_a, query_b, latents, rope_key, key_up_a, value_up_a, key_up_b, value_up_b,
    out_proj_a, out_proj_b, norm_gain, routes, route_weights, shared_gate, shared_up, shared_down,
    expert_gate, expert_up, expert_down,
):
    first_row = lax.axis_index(SP) * TOK
    cosine, sine = tables(first_row + jnp.arange(TOK, dtype=jnp.int32))
    return layer(
        (
            query_a, query_b.T, latents, rope_key.T, cosine, sine, key_up_a.T, key_up_b, value_up_a.T, value_up_b,
            residual, norm_gain.reshape(1, D), routes.T, route_weights.T,
        ),
        (out_proj_a, out_proj_b, shared_gate, shared_up, shared_down, expert_gate[0], expert_up[0], expert_down[0]),
    )


def solution(mesh):
    torus = Mesh(mesh.devices.reshape(NZ, NX, NY, NC), ALL)
    rows, cols, split = P(SP, None), P(None, TP), P(TP, None)
    in_specs = (
        P(SP + TP, None), P(SP, TP), P(SP, TP), rows, rows, cols, cols, cols, cols, split, split, P(), rows, rows,
        cols, cols, split, P(SP, None, TP), P(SP, None, TP), P(SP, TP, None),
    )
    return jax.shard_map(
        shards, mesh=torus, in_specs=in_specs, out_specs=P(SP + TP, None), check_vma=False
    )
```

```python
import functools

import jax
import jax.numpy as jnp
from jax import lax
from jax.experimental import pallas as pl
from jax.experimental.pallas import tpu as pltpu
from jax.sharding import Mesh
from jax.sharding import PartitionSpec as P

DA = 64
VA = 64
DB = 128
VB = 128
ROPE = 32
TOK = 192
D = 2048
W = 128
CAP = 18
CAPP = 24
NZ, NX, NY, NC = 4 * 2, 4, 8, 2
NSP = NZ * NX
NTP = NY * NC
ROWS = NSP * CAP
PROWS = NSP * CAPP
Z_PIECES = 3
PIECES = 4
PIECE = ROWS // PIECES
OWN = TOK // NTP
OWNP = 16
SP = ("z", "x")
TP = ("y", "c")
ALL = ("z", "x", "y", "c")
MESH_ID = pl.DeviceIdType.MESH
F32 = jnp.float32
BF16 = jnp.bfloat16
FAR_FIRST = (4, 3, 5, 2, 6, 1, 7, 0)
MERGED = (4, 2, 6, 1, 7, 3, 5, 0)

theta_base = 10000.0
norm_eps = 1e-06
very_low = -1e30
RATE_A = 1.4426950408889634 * (DA + ROPE) ** (-0.5)
RATE_B = 1.4426950408889634 * (DB + ROPE) ** (-0.5)


def fdot(a, b):
    return jnp.dot(a, b, preferred_element_type=F32)


def rcopy(src, dst, ssem, rsem, dev):
    return pltpu.make_async_remote_copy(
        src_ref=src, dst_ref=dst, send_sem=ssem, recv_sem=rsem, device_id=dev, device_id_type=MESH_ID
    )


def iota(shape, dim):
    return lax.broadcasted_iota(jnp.int32, shape, dim)


def onehot(cond):
    return jnp.where(cond, 1.0, 0.0).astype(BF16)


def lanes(index, width):
    return pl.ds(pl.multiple_of(index * width, 128), width)


def nt(a, b):
    return lax.dot_general(a, b, (((1,), (1,)), ((), ())), preferred_element_type=F32)


def layer_kernel(
    qa, qb_t, lat, rope_t, cosine, sine, kua_t, kub, vua_t, vub,
    resid, gain, routes_t, rw_t,
    oa_h, ob_h, sg_h, su_h, sd_h, eg_h, eu_h, ed_h,
    out_near, out_far,
    lz, q_all, wv_t, m_a, l_a, m_b, l_b, acc_a, acc_b, ps, st, pr, sr, heads, cols8,
    wo, sgu, sd, egu, ed,
    r_s, r_r, own_d, po_d, pi_d, sb_d, rb_d,
    hs, hidden,
    po_s, pi_s, sb_s, rb_s, own_s,
    f_s, f_r, tight, ssq, g, hacc,
    own_i, po_i, pi_i, isb, irb, j_r, l_s, l_r,
    f2_s, f2_r, j2_r, l2_s, l2_r, mg_d, mg_s,
    z_ss, z_rs, zf_ss, zf_rs, zo_ss, zo_rs, q_ss, q_rs, x_ss, x_rs, t_ss, t_rs,
    w_sem, r_ss, r_rs, pd_ss, pd_rs, d_ss, d_rs, e_ss, e_rs, ef_ss, ef_rs,
    ps_ss, ps_rs, s_ss, s_rs, f_ss, f_rs, g_ss, g_rs, gf_ss, gf_rs, go_ss, go_rs,
    pp_ss, pp_rs, i_ss, i_rs, j_ss, j_rs, l_ss, l_rs,
    f2_ss, f2_rs, j2_ss, j2_rs, l2_ss, l2_rs, md_ss, md_rs, ms_ss, ms_rs, g4_ss, g4_rs,
):
    z, x, y, c = (lax.axis_index(a) for a in ALL)
    t = y * NC + c
    t4 = lax.rem(y + 4, NY) * NC + c
    sp = z * NX + x
    oc = 1 - c
    partner = (z, x, y, oc)

    def ydev(yy):
        return (z, x, yy, c)

    def tdev(tt):
        return (z, x, tt // NC, lax.rem(tt, NC))

    def sdev(ss):
        return (ss // NX, lax.rem(ss, NX), y, c)

    def xdev(xx):
        return (z, xx, y, c)

    def zdev(zz):
        return (zz, x, y, c)

    def yoff(off):
        return lax.rem(y + off, NY)

    class Ring:
        def __init__(self, pos, dev, win, pieces, sems, short=False):
            self.short = short
            self.pos, self.dev, self.win, self.pieces = pos, dev, win, pieces
            self.ss, self.rs, self.fs, self.fr, self.os, self.orr = sems

        def src(self, d, k):
            return lax.rem(self.pos + 8 - k, 8) if d == 0 else lax.rem(self.pos + k, 8)

        def to(self, d):
            return self.dev(self.src(1 - d, 1))

        def ok(self, k, d, h):
            return k < 4 or (k == 4 and not self.short and (h < self.pieces // 2) == (d == 0))

        def send(self, d, k, h):
            win = self.win(self.src(d, k - 1), h, c)
            return rcopy(win, win, self.ss.at[d, k - 1, h], self.rs.at[d, k - 1, h], self.to(d))

        def got(self, d, k, h):
            win = self.win(self.src(d, k), h, c)
            return rcopy(win, win, self.ss.at[d, k - 1, h], self.rs.at[d, k - 1, h], self.to(d))

        def fwd(self, d, k, h, core):
            win = self.win(self.src(d, k), h, core)
            return rcopy(win, win, self.fs.at[d, k - 1, h], self.fr.at[d, k - 1, h], partner)

        def own(self, h, core):
            win = self.win(self.pos, h, core)
            return rcopy(win, win, self.os.at[h], self.orr.at[h], partner)

        def pass_on(self, k, d, h):
            if self.ok(k, d, h):
                self.got(d, k, h).wait_recv()
                if self.ok(k + 1, d, h):
                    self.send(d, k + 1, h).start()
                self.fwd(d, k, h, c).start()

        def whole(self, d, k):
            for h in range(self.pieces):
                if self.ok(k, d, h):
                    self.fwd(d, k, h, oc).wait_recv()

        def run(self, use, own_too, after_start, before_use, fourth=None, fourth_end=None):
            half = self.pieces // 2
            for h in range(self.pieces):
                for d in range(2):
                    self.send(d, 1, h).start()
                if own_too:
                    self.own(h, c).start()
            after_start()
            for k in range(1, 5):
                if k == 4 and self.short:
                    fourth()
                for h in range(self.pieces):
                    for d in range(2):
                        self.pass_on(k, d, h)
                    if k > 1 and h == half - 1:
                        self.whole(0, k - 1)
                        use(self.src(0, k - 1), False)
                if k > 1:
                    self.whole(1, k - 1)
                    use(self.src(1, k - 1), False)
                else:
                    before_use()
                    if own_too:
                        for h in range(self.pieces):
                            self.own(h, oc).wait_recv()
                    use(self.pos, True)
            if self.short:
                fourth_end()
            else:
                self.whole(0, 4)
                self.whole(1, 4)
            use(self.src(0, 4), False)

        def finish(self, own_too):
            for h in range(self.pieces):
                if own_too:
                    self.own(h, c).wait_send()
                for k in range(1, 5):
                    for d in range(2):
                        if self.ok(k, d, h):
                            self.send(d, k, h).wait_send()
                            self.fwd(d, k, h, c).wait_send()

    weights = [
        (ob_h, wo.at[0:VB]), (oa_h, wo.at[VB:VB + VA]), (sg_h, sgu.at[:, 0:W]), (su_h, sgu.at[:, W:2 * W]), (sd_h, sd),
        (eg_h, egu.at[:, 0:W]), (eu_h, egu.at[:, W:2 * W]), (ed_h, ed),
    ]
    loads = [pltpu.make_async_copy(a, b, w_sem.at[i]) for i, (a, b) in enumerate(weights)]
    for load in loads:
        load.start()

    barrier = pltpu.get_barrier_semaphore()

    def greet_t(k, _):
        pl.semaphore_signal(barrier, inc=1, device_id=tdev(lax.rem(t + k, NTP)), device_id_type=MESH_ID)
        return 0

    def greet_s(k, _):
        pl.semaphore_signal(barrier, inc=1, device_id=sdev(lax.rem(sp + k, NSP)), device_id_type=MESH_ID)
        return 0

    lax.fori_loop(1, NTP, greet_t, 0)
    lax.fori_loop(1, NSP, greet_s, 0)

    def unit(size):
        return onehot(iota((size, size), 0) == iota((size, size), 1))

    def turn(value):
        wide = value.astype(F32)
        swapped = jnp.concatenate([wide[ROPE // 2:], wide[0:ROPE // 2]], axis=0)
        return (wide * cosine[...] + swapped * sine[...]).astype(BF16)

    unit_tok = unit(TOK)
    rot = turn(rope_t[...])
    lz[z, :, 0:512] = lat[...]
    lz[z, :, 512:640] = nt(unit_tok, jnp.concatenate([jnp.zeros((64, TOK), BF16), rot, rot], axis=0)).astype(BF16)
    qa_t = nt(unit(DA + ROPE), qa[...]).astype(BF16)
    q_t = jnp.concatenate([qb_t[0:DB], qa_t[0:DA], turn(qa_t[DA:DA + ROPE]), turn(qb_t[DB:DB + ROPE])], axis=0)
    q_all[x] = nt(unit_tok, q_t).astype(BF16)
    wv_t[0:VB] = nt(unit(VB), vub[...]).astype(BF16)
    wv_t[VB:VB + VA] = vua_t[...]

    names_t = onehot((iota((128, TOK), 0) == routes_t[0:1, :]) | (iota((128, TOK), 0) == routes_t[1:2, :]))
    upper = onehot(iota((TOK, TOK), 0) < iota((TOK, TOK), 1))
    before_t = fdot(names_t, upper)

    def slot_row(k):
        rank = jnp.sum(jnp.where(iota((128, TOK), 0) == routes_t[k:k + 1, :], before_t, 0.0), axis=0, keepdims=True)
        return routes_t[k:k + 1, :] * CAPP + rank.astype(jnp.int32)

    r_s[...] = jnp.zeros_like(r_s)
    tight[ROWS:, :] = jnp.zeros((8, W), F32)
    r_s[0:OWN, :] = resid[...]

    pl.semaphore_wait(barrier, NTP - 1 + NSP - 1)

    def resid_copy(k, to):
        tt = lax.rem(t + k, NTP) if to else lax.rem(t + NTP - k, NTP)
        return rcopy(r_s.at[:, lanes(tt if to else t, W)], r_r.at[t if to else tt], r_ss.at[k], r_rs.at[k], tdev(tt))

    def resid_send(k, _):
        resid_copy(k, True).start()
        return 0

    r_r[t] = r_s[:, lanes(t, W)]

    def pair_out(value, off, own, po, pi, ss, rs):
        left, right = value[:, 0:W], value[:, W:2 * W]
        own[off] = jnp.where(c == 0, left, right)
        po[off] = jnp.where(c == 0, right, left).astype(BF16)
        rcopy(po.at[off], pi.at[off], ss.at[off], rs.at[off], partner).start()

    def pair_wait(off, po, pi, ss, rs):
        rcopy(po.at[off], pi.at[off], ss.at[off], rs.at[off], partner).wait()

    def y_copy(off, sb, rb, ss, rs):
        return rcopy(sb.at[off], rb.at[off], ss.at[off], rs.at[off], ydev(yoff(off)))

    def merge_copy(i, sb, mg, ms, mr):
        half = sb.at[4, pl.ds(i * (TOK // 2), TOK // 2), :]
        return rcopy(half, mg.at[i], ms.at[i], mr.at[i], ydev(yoff(1 if i == 0 else 7)))

    def scatter_one(off, own, po, pi, sb, rb, pss, prs, ss, rs, mg, ms, mr):
        pair_wait(off, po, pi, pss, prs)
        if off == 0:
            return
        total = own[off] + pi[off].astype(F32)
        if off in (3, 5):
            i = 0 if off == 3 else 1
            merge_copy(i, sb, mg, ms, mr).wait()
            came = mg[i].astype(F32)
            still = jnp.zeros_like(came)
            total = total + jnp.concatenate([came, still] if i == 0 else [still, came], axis=0)
        sb[off] = total.astype(BF16)
        if off == 4:
            for i in range(2):
                merge_copy(i, sb, mg, ms, mr).start()
        else:
            y_copy(off, sb, rb, ss, rs).start()

    def scatter_start(cols, own, po, pi, *rest, lead=3):
        for n in range(NY + lead):
            if n < NY:
                off = MERGED[n]
                pair_out(cols(yoff(off)), off, own, po, pi, rest[2], rest[3])
            if n >= lead:
                scatter_one(MERGED[n - lead], own, po, pi, *rest)

    def scatter_send(offs, *all_of):
        for off in offs:
            scatter_one(off, *all_of)

    def scatter_end(own, pi, sb, rb, ss, rs):
        total = own[0] + pi[0].astype(F32)
        for off in (2, 6, 1, 7, 3, 5):
            y_copy(off, sb, rb, ss, rs).wait()
            total = total + rb[off].astype(F32)
        return total

    def z_win(zz, h, core):
        size = TOK // 2 // Z_PIECES
        start = pl.multiple_of(core * (TOK // 2) + h * size, size)
        return lz.at[zz, pl.ds(start, size), :]

    def q_copy(off, to):
        src = x if to else lax.rem(x + NX - off, NX)
        return rcopy(q_all.at[src], q_all.at[src], q_ss.at[off], q_rs.at[off], xdev(lax.rem(x + off, NX)))

    def queries_here():
        lax.fori_loop(1, NTP, resid_send, 0)
        for off in (2, 1, 3):
            q_copy(off, False).wait_recv()

    def block(zz, first):
        rows = lz[zz]
        part, twice = rows[:, 0:512], rows[:, 512:640].astype(F32)
        lane = iota((TOK, 128), 1)
        keys_b = fdot(part, kub[...])
        keys_a = jnp.concatenate([nt(part, kua_t[...]), twice[:, 64:128]], axis=1)
        keys_a = jnp.where(lane < 96, keys_a, 0.0).astype(BF16)
        keys_b = jnp.concatenate([keys_b, jnp.where(lane < 96, 0.0, twice)], axis=1).astype(BF16)
        values = nt(wv_t[...], part).astype(BF16)
        queries = q_all[...].reshape(NX * TOK, 256)
        if first:
            shape = (TOK, NX * TOK)
            seen = x * TOK + iota(shape, 0) <= iota(shape, 1)
        for scores, rate, m, l, acc, lo, hi in (
            (nt(keys_b, queries), RATE_B, m_b, l_b, acc_b, 0, VB),
            (nt(keys_a, queries[:, 128:256]), RATE_A, m_a, l_a, acc_a, VB, VB + VA),
        ):
            if first:
                scores = jnp.where(seen, scores, very_low)
                top = jnp.max(scores, axis=0, keepdims=True)
                expo = jnp.where(seen, jnp.exp2((scores - top) * rate), 0.0)
                l[...] = jnp.sum(expo, axis=0, keepdims=True)
                acc[...] = fdot(values[lo:hi], expo.astype(BF16))
            else:
                top = jnp.maximum(m[...], jnp.max(scores, axis=0, keepdims=True))
                expo = jnp.exp2((scores - top) * rate)
                fade = jnp.exp2((m[...] - top) * rate)
                l[...] = l[...] * fade + jnp.sum(expo, axis=0, keepdims=True)
                acc[...] = acc[...] * fade + fdot(values[lo:hi], expo.astype(BF16))
            m[...] = top

    def use_block(zz, first):
        if first:
            block(zz, True)
        else:
            pl.when(zz < z)(lambda: block(zz, False))

    z_ring = Ring(z, zdev, z_win, Z_PIECES, (z_ss, z_rs, zf_ss, zf_rs, zo_ss, zo_rs))
    for off in (2, 1, 3):
        q_copy(off, True).start()
    z_ring.run(use_block, False, lambda: None, queries_here)

    share_b = jnp.where(l_b[...] > 0, 1.0 / l_b[...], 0.0)
    share_a = jnp.where(l_a[...] > 0, 1.0 / l_a[...], 0.0)
    out = jnp.concatenate([acc_b[...] * share_b, acc_a[...] * share_a], axis=0).astype(BF16)
    for xx in range(NX):
        cut = slice(xx * TOK, (xx + 1) * TOK)
        one = out[:, cut]
        ps[xx, 0:TOK] = one[:, 0:128]
        ps[xx, TOK:] = jnp.concatenate([one[0:TOK // 2, 128:], one[TOK // 2:, 128:]], axis=1)
        for i, stat in enumerate((m_b, l_b, m_a, l_a)):
            st[xx, i:i + 1, :] = stat[:, cut]
            st[xx, i + 4:i + 5, :] = stat[:, cut]

    def x_copy(src, dst, ss, rs, off, to):
        there = lax.rem(x + off, NX) if to else lax.rem(x + NX - off, NX)
        return rcopy(src.at[there], dst.at[x if to else there], ss.at[off], rs.at[off], xdev(there))

    for off in (2, 1, 3):
        x_copy(st, sr, t_ss, t_rs, off, True).start()
        x_copy(ps, pr, x_ss, x_rs, off, True).start()
    pr[x] = ps[x]
    sr[x] = st[x]
    for load in loads:
        load.wait()
    for i in range(NTP):
        cut = slice(i * W, (i + 1) * W)
        column = jnp.transpose(jnp.broadcast_to(gain[:, cut], (8, W)))[:, 0:1]
        for ref in (sgu, egu):
            ref[cut, :] = (ref[cut, :].astype(F32) * column).astype(BF16)
    for off in range(1, NX):
        x_copy(st, sr, t_ss, t_rs, off, False).wait()
        x_copy(ps, pr, x_ss, x_rs, off, False).wait()
    whole_of = []
    for i in range(NX):
        ends = pr[i, TOK:].astype(F32)
        ends = jnp.concatenate([ends[:, 0:TOK - 128], ends[:, TOK - 128:]], axis=0)
        whole_of.append(jnp.concatenate([pr[i, 0:TOK].astype(F32), ends], axis=1))
    merged = []
    for row, rate, lo, hi in ((0, RATE_B, 0, VB), (2, RATE_A, VB, VB + VA)):
        tops = [sr[i, row:row + 1, :] for i in range(NX)]
        top = functools.reduce(jnp.maximum, tops)
        part = [jnp.exp2((tops[i] - top) * rate) * sr[i, row + 1:row + 2, :] for i in range(NX)]
        whole = 1.0 / sum(part)
        merged.append(sum(whole_of[i][lo:hi] * (part[i] * whole) for i in range(NX)))
    turned = jnp.concatenate(merged, axis=0).astype(BF16)
    heads[...] = nt(unit_tok, turned).astype(BF16)

    def head_cols(yy):
        return fdot(heads[...], wo[:, lanes(yy, 2 * W)])

    scatter_start(head_cols, own_d, po_d, pi_d, sb_d, rb_d, pd_ss, pd_rs, d_ss, d_rs, mg_d, md_ss, md_rs)

    def resid_wait(k, _):
        resid_copy(k, False).wait()
        return 0

    mixed = scatter_end(own_d, pi_d, sb_d, rb_d, d_ss, d_rs)
    lax.fori_loop(1, NTP, resid_wait, 0)
    i12 = iota((TOK, 1), 0)
    pick12 = onehot(iota((TOK, NTP * OWNP), 1) == i12 + (OWNP - OWN) * ((i12 * 5462) >> 16))
    resid_cols = fdot(pick12, r_r[...].reshape(NTP * OWNP, W))
    hs[...] = (resid_cols + mixed).astype(BF16)

    place = onehot((iota((PROWS, TOK), 0) == slot_row(0)) | (iota((PROWS, TOK), 0) == slot_row(1)))

    f_s[...] = fdot(place, hs[...]).reshape(NSP, CAPP, W).astype(BF16)
    f_r[sp] = f_s[sp]

    def far_first(i):
        odd = lax.rem(i, 2)
        return NSP // 2 + odd * ((i + 1) // 2) - (1 - odd) * (i // 2)

    def sp_copy(k, src, dst, ss, rs, to):
        peer = lax.rem(sp + k, NSP) if to else lax.rem(sp + NSP - k, NSP)
        return rcopy(src.at[peer], dst.at[sp if to else peer], ss.at[k], rs.at[k], sdev(peer))

    def f_send(k, _):
        sp_copy(k, f_s, f_r, f_ss, f_rs, True).start()
        return 0

    def f_wait(k, _):
        sp_copy(k, f_s, f_r, f_ss, f_rs, False).wait()
        return 0

    lax.fori_loop(0, NSP - 1, lambda i, _: f_send(far_first(i), 0), 0)

    hidden[:, lanes(t, W)] = hs[...]

    def e_copy(off):
        return rcopy(hs, hidden.at[:, lanes(t, W)], e_ss.at[off], e_rs.at[off], ydev(yoff(off)))

    def e_got(off):
        src = lanes(lax.rem(y + NY - off, NY) * NC + c, W)
        return rcopy(hs, hidden.at[:, src], e_ss.at[off], e_rs.at[off], ydev(yoff(off)))

    def e_fwd(off, core):
        win = hidden.at[:, lanes(lax.rem(y + NY - off, NY) * NC + core, W)]
        return rcopy(win, win, ef_ss.at[off], ef_rs.at[off], partner)

    for off in FAR_FIRST[:-1]:
        e_copy(off).start()
    e_fwd(0, c).start()

    def f2_send(k, _):
        sp_copy(k, f2_s, f2_r, f2_ss, f2_rs, True).start()
        return 0

    def f2_wait(k, _):
        sp_copy(k, f2_s, f2_r, f2_ss, f2_rs, False).wait()
        return 0

    lax.fori_loop(1, NSP, f_wait, 0)
    for e in range(NSP):
        tight[e * CAP:e * CAP + CAPP, :] = f_r[e].astype(F32)
    g[y, :, lanes(c, W)] = tight[0:ROWS, :].astype(BF16)

    def g_win(yy, h, core):
        return g.at[yy, pl.ds(h * PIECE, PIECE), lanes(core, W)]

    def gate_up(yy, first):
        wide = g[yy].astype(F32)
        wide = wide * wide
        squares = wide[:, 0:W] + wide[:, W:2 * W]
        ssq[...] = squares if first else ssq[...] + squares
        value = fdot(g[yy], egu[pl.ds(pl.multiple_of(yy * 2 * W, 2 * W), 2 * W), :])
        hacc[...] = value if first else hacc[...] + value

    y_ring = Ring(y, ydev, g_win, PIECES, (g_ss, g_rs, gf_ss, gf_rs, go_ss, go_rs), True)
    def hidden_relay():
        e_got(4).wait_recv()
        f2_s[...] = fdot(place, hidden[:, lanes(t4, W)]).reshape(NSP, CAPP, W).astype(BF16)
        f2_r[sp] = f2_s[sp]
        lax.fori_loop(0, NSP - 1, lambda i, _: f2_send(far_first(i), 0), 0)
        e_fwd(4, c).start()
        for off in (1, 7, 2, 6, 3, 5):
            e_got(off).wait_recv()
            e_fwd(off, c).start()

    def root(total):
        return lax.rsqrt(jnp.sum(total, axis=1, keepdims=True) * (1.0 / D) + norm_eps)

    def gated(both, scale):
        gate, up = both[:, 0:W] * scale, both[:, W:2 * W] * scale
        return (gate / (1.0 + jnp.exp(-gate)) * up).astype(BF16)

    def shared_pairs():
        for off in range(NY):
            e_fwd(off, oc).wait_recv()
        total = jnp.zeros((TOK, W), F32)
        for i in range(NTP):
            wide = hidden[:, i * W:(i + 1) * W].astype(F32)
            total = total + wide * wide
        shared_act = gated(fdot(hidden[...], sgu[...]), root(total))
        for off in range(NY):
            value = fdot(shared_act, sd[:, lanes(yoff(off), 2 * W)])
            pair_out(value, off, own_s, po_s, pi_s, ps_ss, ps_rs)

    def g_four(core):
        win = g.at[yoff(4), :, lanes(core, W)]
        return rcopy(win, win, g4_ss, g4_rs, partner)

    def fourth():
        lax.fori_loop(1, NSP, f2_wait, 0)
        for e in range(NSP):
            tight[e * CAP:e * CAP + CAPP, :] = f2_r[e].astype(F32)
        g[yoff(4), :, lanes(c, W)] = tight[0:ROWS, :].astype(BF16)
        g_four(c).start()
        scatter_send((4, 2, 6), own_s, po_s, pi_s, sb_s, rb_s, ps_ss, ps_rs, s_ss, s_rs, mg_s, ms_ss, ms_rs)

    y_ring.run(gate_up, True, hidden_relay, shared_pairs, fourth, lambda: g_four(oc).wait_recv())
    act = gated(hacc[...], root(ssq[...]))

    def i_pair(off):
        pair_out(fdot(act, ed[:, lanes(yoff(off), 2 * W)]), off, own_i, po_i, pi_i, pp_ss, pp_rs)

    def i_copy(d, k, h):
        return rcopy(isb.at[d, k - 1, h], irb.at[d, k - 1, h], i_ss.at[d, k - 1, h], i_rs.at[d, k - 1, h], y_ring.to(d))

    def i_step(k):
        for h in range(PIECES):
            for d in range(2):
                off = (4 - k) if d == 0 else (4 + k)
                rows = pl.ds(h * PIECE, PIECE)
                total = own_i[off, rows, :] + pi_i[off, rows, :].astype(F32)
                if k > 1:
                    i_copy(d, k - 1, h).wait_recv()
                    total = total + irb[d, k - 2, h].astype(F32)
                isb[d, k - 1, h] = total.astype(BF16)
                i_copy(d, k, h).start()

    def i_wait(*offs):
        for off in offs:
            pair_wait(off, po_i, pi_i, pp_ss, pp_rs)

    i_pair(3)
    i_pair(5)
    i_pair(4)
    i_pair(2)
    i_wait(3, 5)
    i_step(1)
    i_pair(6)
    i_wait(4)
    tight[0:ROWS, :] = own_i[4] + pi_i[4].astype(F32)
    for e in range(NSP):
        f2_s[e] = tight[e * CAP:e * CAP + CAPP, :].astype(BF16)
    j2_r[sp] = f2_s[sp]

    def j2_send(k, _):
        sp_copy(k, f2_s, j2_r, j2_ss, j2_rs, True).start()
        return 0

    def j2_wait(k, _):
        sp_copy(k, f2_s, j2_r, j2_ss, j2_rs, False).wait()
        return 0

    lax.fori_loop(0, NSP - 1, lambda i, _: j2_send(far_first(i), 0), 0)
    i_wait(2, 6)
    i_step(2)
    i_pair(1)
    i_pair(7)
    i_pair(0)
    i_wait(1, 7)
    i_step(3)
    i_wait(0)
    for h in range(PIECES):
        rows = pl.ds(h * PIECE, PIECE)
        total = own_i[0, rows, :] + pi_i[0, rows, :].astype(F32)
        for d in range(2):
            i_copy(d, 3, h).wait_recv()
            total = total + irb[d, 2, h].astype(F32)
        tight[rows, :] = total

    for e in range(NSP):
        f_s[e] = tight[e * CAP:e * CAP + CAPP, :].astype(BF16)
    j_r[sp] = f_s[sp]

    def j_send(k, _):
        sp_copy(k, f_s, j_r, j_ss, j_rs, True).start()
        return 0

    def j_wait(k, _):
        sp_copy(k, f_s, j_r, j_ss, j_rs, False).wait()
        return 0

    lax.fori_loop(0, NSP - 1, lambda i, _: j_send(far_first(i), 0), 0)
    scatter_send((3, 5, 1, 7, 0), own_s, po_s, pi_s, sb_s, rb_s, ps_ss, ps_rs, s_ss, s_rs, mg_s, ms_ss, ms_rs)
    rows8 = jnp.concatenate(
        [slot_row(0).astype(F32), slot_row(1).astype(F32), rw_t[0:1, :], rw_t[1:2, :], jnp.zeros((4, TOK), F32)], axis=0
    )
    cols8[...] = jnp.transpose(rows8)
    j16 = iota((NTP * OWNP, 1), 0)
    spread = onehot(iota((NTP * OWNP, TOK), 1) == jnp.where((j16 & 15) < OWN, OWN * (j16 >> 4) + (j16 & 15), -1))
    picks = [onehot(iota((TOK, PROWS), 1) == cols8[:, k:k + 1].astype(jnp.int32)) for k in range(2)]

    def routed(ref):
        back = ref[...].astype(F32).reshape(PROWS, W).astype(BF16)
        return sum(fdot(picks[k], back) * cols8[:, k + 2:k + 3] for k in range(2))

    def to_rows(value, l_s, l_r, window, ss, rs):
        l_s[...] = fdot(spread, value.astype(BF16)).astype(BF16).reshape(NTP, OWNP, W)
        l_r[:, lanes(window(t), W)] = l_s[t]

        def l_send(k, _):
            l_copy(k, True, l_s, l_r, window, ss, rs).start()
            return 0

        lax.fori_loop(1, NTP, l_send, 0)

    def l_copy(k, to, l_s, l_r, window, ss, rs):
        tt = lax.rem(t + k, NTP) if to else lax.rem(t + NTP - k, NTP)
        return rcopy(l_s.at[tt], l_r.at[:, lanes(window(t if to else tt), W)], ss.at[k], rs.at[k], tdev(tt))

    def near(tt):
        return tt

    def far(tt):
        return lax.rem(tt + NTP // 2, NTP)

    lax.fori_loop(1, NSP, j2_wait, 0)
    to_rows(routed(j2_r), l2_s, l2_r, far, l2_ss, l2_rs)
    final = hs[...].astype(F32) + scatter_end(own_s, pi_s, sb_s, rb_s, s_ss, s_rs)
    lax.fori_loop(1, NSP, j_wait, 0)
    to_rows(final + routed(j_r), l_s, l_r, near, l_ss, l_rs)

    def l_wait(k, _):
        l_copy(k, False, l2_s, l2_r, far, l2_ss, l2_rs).wait()
        l_copy(k, False, l_s, l_r, near, l_ss, l_rs).wait()
        return 0

    for off in range(1, NY):
        e_copy(off).wait_send()
    for off in range(NY):
        e_fwd(off, c).wait_send()
    z_ring.finish(False)
    g_four(c).wait_send()
    y_ring.finish(True)
    for off in range(1, NX):
        q_copy(off, True).wait_send()
    for k in range(1, 4):
        for h in range(PIECES):
            for d in range(2):
                i_copy(d, k, h).wait_send()
    lax.fori_loop(1, NTP, l_wait, 0)
    out_near[...] = l_r[0:OWN, :]
    out_far[...] = l2_r[0:OWN, :]


def layer(vmem_args, hbm_args):
    dma = pltpu.SemaphoreType.DMA
    vm = pltpu.VMEM
    row = vm((1, NX * TOK), F32)
    zsem, ysem = (2, 4, Z_PIECES), (2, 4, PIECES)
    scratch = [
        vm((NZ, TOK, 640), BF16), vm((NX, TOK, 256), BF16), vm((VA + VB, 512), BF16), row, row, row, row,
        vm((VA, NX * TOK), F32), vm((VB, NX * TOK), F32), vm((NX, TOK + TOK // 2, 128), BF16), vm((NX, 8, TOK), F32),
        vm((NX, TOK + TOK // 2, 128), BF16), vm((NX, 8, TOK), F32), vm((TOK, VA + VB), BF16), vm((TOK, 8), F32),
        vm((VA + VB, D), BF16), vm((D, 2 * W), BF16), vm((W, D), BF16), vm((D, 2 * W), BF16), vm((W, D), BF16),
        vm((OWNP, D), BF16), vm((NTP, OWNP, W), BF16),
        vm((NY, TOK, W), F32), vm((NY, TOK, W), BF16), vm((NY, TOK, W), BF16), vm((NY, TOK, W), BF16), vm((NY, TOK, W), BF16),
        vm((TOK, W), BF16), vm((TOK, D), BF16),
        vm((NY, TOK, W), BF16), vm((NY, TOK, W), BF16), vm((NY, TOK, W), BF16), vm((NY, TOK, W), BF16), vm((NY, TOK, W), F32),
        vm((NSP, CAPP, W), BF16), vm((NSP, CAPP, W), BF16), vm((ROWS + 8, W), F32), vm((ROWS, W), F32), vm((NY, ROWS, 2 * W), BF16), vm((ROWS, 2 * W), F32),
        vm((NY, ROWS, W), F32), vm((NY, ROWS, W), BF16), vm((NY, ROWS, W), BF16), vm((2, 4, PIECES, PIECE, W), BF16), vm((2, 4, PIECES, PIECE, W), BF16),
        vm((NSP, CAPP, W), BF16), vm((NTP, OWNP, W), BF16), vm((OWNP, D), BF16),
        vm((NSP, CAPP, W), BF16), vm((NSP, CAPP, W), BF16), vm((NSP, CAPP, W), BF16), vm((NTP, OWNP, W), BF16), vm((OWNP, D), BF16),
        vm((2, TOK // 2, W), BF16), vm((2, TOK // 2, W), BF16),
    ] + [
        dma(n) for n in (
            zsem, zsem, zsem, zsem, (2,), (2,), (NX,), (NX,), (NX,), (NX,), (NX,), (NX,),
            (8,), (NTP,), (NTP,), (NY,), (NY,), (NY,), (NY,), (NY,), (NY,), (NY,), (NY,),
            (NY,), (NY,), (NY,), (NY,), (NSP,), (NSP,),
            ysem, ysem, ysem, ysem, (PIECES,), (PIECES,),
            (NY,), (NY,), ysem, ysem, (NSP,), (NSP,), (NTP,), (NTP,),
            (NSP,), (NSP,), (NSP,), (NSP,), (NTP,), (NTP,), (2,), (2,), (2,), (2,),
        )
    ] + [dma, dma]
    vspec = pl.BlockSpec(memory_space=pltpu.VMEM)
    hspec = pl.BlockSpec(memory_space=pl.ANY)
    near, far = pl.pallas_call(
        layer_kernel,
        out_shape=[jax.ShapeDtypeStruct((OWN, D), BF16)] * 2,
        in_specs=[vspec] * len(vmem_args) + [hspec] * len(hbm_args),
        out_specs=[vspec] * 2,
        scratch_shapes=scratch,
        compiler_params=pltpu.CompilerParams(collective_id=1, has_side_effects=True, vmem_limit_bytes=60 * 2**20),
        name="layer",
    )(*vmem_args, *hbm_args)
    return (near.astype(F32) + far.astype(F32)).astype(BF16)


def tables(positions):
    freqs = theta_base ** (-(2.0 * jnp.arange(ROPE // 2, dtype=F32)) / ROPE)
    angles = positions.astype(F32)[None, :] * freqs[:, None]
    cosine, sine = jnp.cos(angles), jnp.sin(angles)
    return jnp.concatenate([cosine, cosine], axis=0), jnp.concatenate([-sine, sine], axis=0)


def shards(
    residual, query_a, query_b, latents, rope_key, key_up_a, value_up_a, key_up_b, value_up_b,
    out_proj_a, out_proj_b, norm_gain, routes, route_weights, shared_gate, shared_up, shared_down,
    expert_gate, expert_up, expert_down,
):
    first_row = lax.axis_index(SP) * TOK
    cosine, sine = tables(first_row + jnp.arange(TOK, dtype=jnp.int32))
    return layer(
        (
            query_a, query_b.T, latents, rope_key.T, cosine, sine, key_up_a.T, key_up_b, value_up_a.T, value_up_b,
            residual, norm_gain.reshape(1, D), routes.T, route_weights.T,
        ),
        (out_proj_a, out_proj_b, shared_gate, shared_up, shared_down, expert_gate[0], expert_up[0], expert_down[0]),
    )


def solution(mesh):
    torus = Mesh(mesh.devices.reshape(NZ, NX, NY, NC), ALL)
    rows, cols, split = P(SP, None), P(None, TP), P(TP, None)
    in_specs = (
        P(SP + TP, None), P(SP, TP), P(SP, TP), rows, rows, cols, cols, cols, cols, split, split, P(), rows, rows,
        cols, cols, split, P(SP, None, TP), P(SP, None, TP), P(SP, TP, None),
    )
    return jax.shard_map(
        shards, mesh=torus, in_specs=in_specs, out_specs=P(SP + TP, None), check_vma=False
    )
```
